32 devices in a mesh: sp: 8 (over z, x), dp: 4 (over y, core).
Axes of the slice: x: 2, y: 2, z: 4, core: 2. Of those that a mesh axis runs over, the one named last changes fastest.
Arguments:
- tokens: bfloat16 [32, 512, 2048], P('dp', 'sp'), may hold values from -6 to 6
- pre_gain: float32 [2048], replicated, may hold values from 0.1 to 1.9
- w_query: bfloat16 [2048, 512], P('dp'), may hold values from -0.125 to 0.125
- w_forget: bfloat16 [2048, 512], P('dp'), may hold values from -0.125 to 0.125
- w_value: bfloat16 [2048, 512], P('dp'), may hold values from -0.125 to 0.125
- w_gate: bfloat16 [2048, 512], P('dp'), may hold values from -0.125 to 0.125
- lower_bound: float32 [512], replicated, may hold values from 0.8 to 1
- extra_decay: float32 [128, 512], P(('dp', 'sp')), may hold values from -1.5 to 0
- initial_state: float32 [128, 128, 128], P(('dp', 'sp')), may hold values from -0.18 to 0.18
- norm_gain: float32 [128], replicated, may hold values from 0.1 to 1.9
- w_out: bfloat16 [512, 2048], P('dp'), may hold values from -0.25 to 0.25
- post_gain: float32 [2048], replicated, may hold values from 0.1 to 1.9
Outputs:
- layer_out: bfloat16 [32, 512, 2048], P('dp', 'sp')
The draws below stay inside these ranges and needn't reach their ends.
All inputs are finite; a program needn't handle non-finite values.
Results may differ from the reference program's by a relative error of at most 0.015.
Values may be sent and summed in bfloat16 or wider, within the bound.
A program may use at most 64 MiB of HBM per device.

```python
import math
import jax
import jax.numpy as jnp
from jax import lax

D = 2048
HEADS = 4
HK = 128
HV = 128
BLOCK = 64
LOC = 64
SEQUENCE_LENGTH = 512
SEQS = 32


def draw_lower_bound(key, part):
    key_rows = jax.random.split(jax.random.fold_in(key, 11), 4)
    order = jax.random.permutation(key_rows[0], HEADS)
    fast_count = HEADS // 2
    fast_heads = order < fast_count
    slow_gap = jax.random.uniform(key_rows[1], (HEADS, 1), jnp.float32, 0.1, 0.5) / SEQUENCE_LENGTH
    fast_gap = jnp.exp(jax.random.uniform(key_rows[2], (HEADS, 1), jnp.float32, math.log(1.0 / 40.0), math.log(1.0 / 15.0)))
    spread = jnp.exp(jax.random.uniform(key_rows[3], (HEADS, HK), jnp.float32, math.log(0.5), math.log(2.0)))
    forget_gap = jnp.where(fast_heads[:, None], fast_gap, slow_gap) * spread
    return (1.0 - forget_gap).reshape(HEADS * HK)


def draw_extra_decay(key, part):
    key_rows = jax.random.split(jax.random.fold_in(key, 23), 3)
    count_of_rows = SEQS * HEADS
    block_count = SEQUENCE_LENGTH // LOC
    rate_low = 0.3
    rates = jnp.exp(jax.random.uniform(key_rows[0], (count_of_rows, block_count), jnp.float32, math.log(rate_low), math.log(1.2))) / SEQUENCE_LENGTH
    base_offset = -jnp.repeat(rates, LOC, axis=1)
    spike_position = jax.random.randint(key_rows[1], (count_of_rows, 2), 0, SEQUENCE_LENGTH)
    spike_fraction = jax.random.uniform(key_rows[2], (count_of_rows, 2), jnp.float32, 0.2, 0.5)
    token_position = jnp.arange(SEQUENCE_LENGTH, dtype=jnp.int32)
    match_count = token_position[None, None, :] == spike_position[:, :, None]
    spike_events = jnp.sum(jnp.where(match_count, jnp.log1p(-spike_fraction)[:, :, None], 0.0), axis=1)
    return base_offset + spike_events


def block_levels(own_key, extent, cuts, low, largest):
    factor_of, own = 1.0, jax.random.fold_in(own_key, 6)
    for position, parts in cuts:
        draws = jnp.exp(jax.random.uniform(jax.random.fold_in(own, position), (parts,), jnp.float32, low / len(cuts), largest / len(cuts)))
        factor_of = factor_of * jnp.repeat(draws, extent[position] // parts).reshape([-1 if axis == position else 1 for axis in range(len(extent))])
    return factor_of


def scatter_about(key, dims, width, bound, cuts=(), held_as=jnp.bfloat16):
    level = block_levels(key, dims, cuts, -0.22, 0.18) if cuts else 1.0
    entries = jax.random.normal(key, dims, jnp.float32) * width * level
    return jnp.minimum(jnp.maximum(entries, -bound), bound).astype(held_as)


def setup_inputs(seed: int = 0) -> dict:
    key_of = jax.random.split(jax.random.key(seed), 13)
    return {
        "tokens": scatter_about(key_of[0], (SEQS, SEQUENCE_LENGTH, D), 1.0, 6.0, ((0, 4), (1, 8))),
        "pre_gain": jnp.clip(1.0 + 0.18 * jax.random.normal(key_of[1], (D,), jnp.float32), 0.1, 1.9),
        "w_query": scatter_about(key_of[2], (D, HEADS * HK), D ** -0.5, 0.125, ((0, 4),)),
        "w_forget": scatter_about(key_of[3], (D, HEADS * HK), D ** -0.5, 0.125, ((0, 4),)),
        "w_value": scatter_about(key_of[4], (D, HEADS * HV), D ** -0.5, 0.125, ((0, 4),)),
        "w_gate": scatter_about(key_of[5], (D, HEADS * HV), D ** -0.5, 0.125, ((0, 4),)),
        "lower_bound": draw_lower_bound(jax.random.fold_in(key_of[12], 71), 0),
        "extra_decay": draw_extra_decay(jax.random.fold_in(key_of[12], 71), 0),
        "initial_state": scatter_about(key_of[8], (SEQS * HEADS, HK, HV), 0.03, 0.18, ((0, 32),), jnp.float32),
        "norm_gain": jnp.clip(1.0 + 0.18 * jax.random.normal(key_of[9], (HV,), jnp.float32), 0.1, 1.9),
        "w_out": scatter_about(key_of[10], (HEADS * HV, D), (HEADS * HV) ** -0.5, 0.25, ((0, 4),)),
        "post_gain": jnp.clip(1.0 + 0.18 * jax.random.normal(key_of[11], (D,), jnp.float32), 0.1, 1.9),
    }


EPS = 1e-06

def rms_scale(matrix, gain):
    widened = matrix.astype(jnp.float32)
    return widened * lax.rsqrt(lax.optimization_barrier(jnp.mean(widened * widened, axis=-1, keepdims=True)) + EPS) * gain

def recur_item(queries, keys_in, values, log_decay, state_zero):
    length = queries.shape[0]
    block_count = length // BLOCK

    def blocks(matrix):
        return matrix.reshape(block_count, BLOCK, matrix.shape[-1])
    causal_mask = jnp.tril(jnp.ones((BLOCK, BLOCK), dtype=bool))[:, :, None]

    def block_step(carried_state, inputs):
        query_block, key_block, value_block, decay_block = inputs
        cumulative = jnp.cumsum(decay_block, axis=0)
        carried = jnp.dot(query_block * jnp.exp(cumulative), carried_state, precision=lax.Precision.HIGHEST)
        log_gaps = cumulative[:, None, :] - cumulative[None, :, :]
        decay_weight = jnp.where(causal_mask, jnp.exp(jnp.minimum(log_gaps, 0.0)), 0.0)
        scores = jnp.einsum('tk,sk,tsk->ts', query_block, key_block, decay_weight, precision=lax.Precision.HIGHEST)
        within = jnp.dot(scores, value_block, precision=lax.Precision.HIGHEST)
        block_end = cumulative[-1]
        added_state = jnp.dot((key_block * jnp.exp(block_end[None, :] - cumulative)).T, value_block, precision=lax.Precision.HIGHEST)
        return (jnp.exp(block_end)[:, None] * carried_state + added_state, carried + within)
    _, block_outs = lax.scan(block_step, state_zero, (blocks(queries), blocks(keys_in), blocks(values), blocks(log_decay)))
    return block_outs.reshape(length, values.shape[-1])

def reference(tokens, pre_gain, w_query, w_forget, w_value, w_gate, lower_bound, extra_decay, initial_state, norm_gain, w_out, post_gain):
    forget_gap = (1.0 - lower_bound).reshape(HEADS, HK)
    states = initial_state.reshape(SEQS, HEADS, HK, HV)
    extras = extra_decay.reshape(SEQS, HEADS, SEQUENCE_LENGTH)
    query_weight = w_query.reshape(D, HEADS, HK).astype(jnp.float32)
    forget_weight = w_forget.reshape(D, HEADS, HK).astype(jnp.float32)
    value_weight = w_value.reshape(D, HEADS, HV).astype(jnp.float32)
    gate_weight = w_gate.reshape(D, HEADS, HV).astype(jnp.float32)
    out_weight = w_out.reshape(HEADS, HV, D).astype(jnp.float32)

    def one_sequence(inputs):
        row_block, state_zero, extra_rows = inputs
        norm_result = rms_scale(row_block, pre_gain).astype(jnp.bfloat16).astype(jnp.float32)
        q_pre = jnp.einsum('ld,dhk->hlk', norm_result, query_weight).astype(jnp.bfloat16)
        f_pre = jnp.einsum('ld,dhk->hlk', norm_result, forget_weight).astype(jnp.bfloat16)
        v_pre = jnp.einsum('ld,dhk->hlk', norm_result, value_weight).astype(jnp.bfloat16)
        g_pre = jnp.einsum('ld,dhk->hlk', norm_result, gate_weight).astype(jnp.bfloat16)
        queries = jax.nn.silu(q_pre.astype(jnp.float32))
        keys_in = forget_gap[:, None, :] * jax.nn.sigmoid(-f_pre.astype(jnp.float32))
        log_decay = jnp.log1p(-keys_in) + extra_rows[:, :, None]
        values = v_pre.astype(jnp.float32)
        outputs = jax.vmap(recur_item)(queries, keys_in, values, log_decay, state_zero)
        head_normed = (outputs * lax.rsqrt(lax.optimization_barrier(jnp.mean(outputs * outputs, axis=-1, keepdims=True)) + EPS) * norm_gain).astype(jnp.bfloat16)
        head_normed = lax.optimization_barrier(head_normed)
        gated = (head_normed.astype(jnp.float32) * jax.nn.silu(g_pre.astype(jnp.float32))).astype(jnp.bfloat16)
        mixed = jnp.einsum('hlv,hvd->ld', gated.astype(jnp.float32), out_weight)
        return rms_scale(mixed, post_gain).astype(jnp.bfloat16)
    return lax.map(one_sequence, (tokens, states, extras))
```

```python
import functools

import jax
import jax.numpy as jnp
from jax import lax
from jax.experimental import pallas as pl
from jax.experimental.pallas import tpu as pltpu
from jax.sharding import PartitionSpec as P

EPS = 1e-06
MESH = pl.DeviceIdType.MESH
NT = (((1,), (1,)), ((), ()))
TN = (((0,), (0,)), ((), ()))


def rms_scale(matrix, gain):
    widened = matrix.astype(jnp.float32)
    return widened * lax.rsqrt(jnp.mean(widened * widened, axis=-1, keepdims=True) + EPS) * gain


def layer_kernel(
    n,
    ways,
    heads,
    axes,
    tokens_hbm,
    pre_hbm,
    wf_hbm,
    wv_hbm,
    wq_hbm,
    wg_hbm,
    wo_hbm,
    extra_hbm,
    bound_hbm,
    init_hbm,
    gain_hbm,
    post_hbm,
    out_ref,
    *scratch,
):
    units = len(axes)
    groups = heads // 2
    wholes = scratch[:units]
    (
        tokens_ref,
        pre_ref,
        raw_ref,
        bound_ref,
        start_ref,
        gain_ref,
        post_ref,
        normed,
        f_ref,
        v_ref,
        q_ref,
        g_ref,
        keys_ref,
        rel_ref,
        emid_ref,
        eend_ref,
        within_ref,
        gated_ref,
        mixed_ref,
        esend,
        erecv,
        extra_ref,
        isend,
        st,
        fin,
        bb,
        bs,
        ob,
        dbuf,
        dsend,
        local_sem,
        y_send,
        y_recv,
        r_send,
        r_recv,
        s_send,
        s_recv,
        e_send,
        e_recv,
        i_send,
        b_send,
        b_recv,
        d_send,
        d_recv,
        c_send,
        c_recv,
        t_send,
        t_recv,
    ) = scratch[units:]
    me = lax.axis_index("sp")
    rank = lax.axis_index("dp")
    seqs, length, width = tokens_ref.shape
    own, hk, hv = start_ref.shape
    half = 2 * hk
    cols = heads * hk
    total = groups * seqs
    levels = n // 2
    side = lax.rem(me, 2)
    level = me // 2
    parity = lax.rem(level, 2)
    beside = me + 1 - 2 * side
    across = me + 2 - 4 * parity
    sibling = rank + 1 - 2 * lax.rem(rank, 2)
    peers = ways // 2 - 1
    unit_q, unit_g, unit_o = 2 * groups, 2 * groups + 1, 2 * groups + 2

    def source(u):
        if u < 2 * groups:
            base = wf_hbm if u % 2 == 0 else wv_hbm
            return base.at[:, (u // 2) * half : (u // 2 + 1) * half]
        return (wq_hbm, wg_hbm, wo_hbm)[u - 2 * groups]

    def full(u, shard):
        rows = wholes[u].shape[0] // ways
        return wholes[u].at[pl.ds(pl.multiple_of(shard * rows, rows), rows)]

    def part(u, shard, which):
        rows = wholes[u].shape[0] // ways
        start = shard * rows + which * (rows // 2)
        return wholes[u].at[pl.ds(pl.multiple_of(start, rows // 2), rows // 2)]

    def local_copy(u):
        return pltpu.make_async_copy(source(u), full(u, rank), local_sem.at[u])

    small = [
        pltpu.make_async_copy(src, dst, local_sem.at[units + j])
        for j, (src, dst) in enumerate(
            (
                (extra_hbm, raw_ref),
                (init_hbm, start_ref),
                (tokens_hbm, tokens_ref),
                (pre_hbm, pre_ref),
                (bound_hbm, bound_ref),
                (gain_hbm, gain_ref),
                (post_hbm, post_ref),
            )
        )
    ]
    local_copy(0).start()
    for copy in small:
        copy.start()
    for u in range(1, units):
        local_copy(u).start()

    barrier = pltpu.get_barrier_semaphore()
    for offset in range(1, n):
        pl.semaphore_signal(
            barrier, inc=1, device_id={"sp": lax.rem(me + offset, n)}, device_id_type=MESH
        )
    for offset in range(1, ways):
        pl.semaphore_signal(
            barrier, inc=1, device_id={"dp": lax.rem(rank + offset, ways)}, device_id_type=MESH
        )
    pl.semaphore_wait(barrier, n + ways - 2)

    def remote(src, dst, send, recv, device):
        return pltpu.make_async_remote_copy(
            src_ref=src,
            dst_ref=dst,
            send_sem=send,
            recv_sem=recv,
            device_id=device,
            device_id_type=MESH,
        )

    def which(u):
        return side if axes[u] == "x" else parity

    def first_part(u, shard):
        return full(u, shard) if axes[u] is None else part(u, shard, which(u))

    def y_copy(u, k):
        ref = first_part(u, rank)
        target = lax.rem(rank + 2 * (k + 1), ways)
        return remote(ref, ref, y_send.at[u, k], y_recv.at[u, k], {"dp": target})

    def origin(k):
        return lax.rem(rank + ways - 2 * (k + 1), ways)

    def r_copy(u, k):
        ref = part(u, origin(k), which(u))
        device = {"sp": beside if axes[u] == "x" else across}
        return remote(ref, ref, r_send.at[u, k], r_recv.at[u, k], device)

    def s_own(u):
        ref = full(u, rank)
        return remote(ref, ref, s_send.at[u, 0], s_recv.at[u, 0], {"dp": sibling})

    def s_copy(u, k, second):
        ref = part(u, origin(k), 1 - which(u)) if second else first_part(u, origin(k))
        slot = 1 + 2 * k + second
        return remote(ref, ref, s_send.at[u, slot], s_recv.at[u, slot], {"dp": sibling})

    def pass_y(u):
        for k in range(peers):
            y_copy(u, k).wait_recv()
            if axes[u] is not None:
                r_copy(u, k).start()
            s_copy(u, k, 0).start()

    def pass_r(u):
        if axes[u] is None:
            return
        for k in range(peers):
            r_copy(u, k).wait_recv()
            s_copy(u, k, 1).start()

    def arrived(u):
        s_own(u).wait_recv()
        for k in range(peers):
            s_copy(u, k, 0).wait_recv()
            if axes[u] is not None:
                s_copy(u, k, 1).wait_recv()

    def e_copy(offset):
        target = lax.rem(me + offset, n)
        return remote(
            esend.at[target],
            erecv.at[me],
            e_send.at[offset - 1],
            e_recv.at[offset - 1],
            {"sp": target},
        )

    def place(j):
        it = me * own + j
        h = lax.rem(it, heads)
        return lax.rem(h, 2), (h // 2) * seqs + it // heads

    def i_copy(j):
        target, k = place(j)
        return remote(isend.at[j], st.at[k, 0], i_send.at[j], c_recv.at[k], {"sp": target})

    def b_copy(k):
        return remote(bs.at[k], bb.at[k, side], b_send.at[k], b_recv.at[k], {"sp": beside})

    def d_copy(g):
        return remote(dsend.at[g], dbuf.at[side, g], d_send.at[g], d_recv.at[g], {"sp": beside})

    def c_copy(k):
        target = lax.rem(me + 2, n)
        return remote(ob.at[k], st.at[k, 0], c_send.at[k], c_recv.at[k], {"sp": target})

    def t_copy(k):
        return remote(st.at[k, 1 - side], fin.at[k], t_send.at[k], t_recv.at[k], {"sp": beside})

    for u in range(units):
        local_copy(u).wait()
        for k in range(peers):
            y_copy(u, k).start()
        s_own(u).start()
    for copy in small:
        copy.wait()

    pad = esend.shape[2]
    for p in range(n):
        piece = raw_ref[:, p * length : (p + 1) * length]
        esend[p] = jnp.concatenate(
            [piece, jnp.zeros((own, pad - length), jnp.float32)], axis=1
        )
    for offset in range(1, n):
        e_copy(offset).start()
    for j in range(own):
        isend[j] = start_ref[j].T.astype(jnp.bfloat16)
    for j in range(own):
        target, k = place(j)

        @pl.when(me != target)
        def _():
            i_copy(j).start()

        @pl.when(me == target)
        def _():
            st[k, 0] = isend[j]

    def norm_rows(s, carry):
        rows = pl.ds(pl.multiple_of(s * length, length), length)
        normed[rows, :] = rms_scale(tokens_ref[s], pre_ref[...]).astype(jnp.bfloat16)
        return carry

    lax.fori_loop(0, seqs, norm_rows, 0)
    erecv[me] = esend[me]
    for offset in range(1, n):
        e_copy(offset).wait_recv()

    def turn(p, carry):
        extra_ref[p] = erecv[p].T
        return carry

    lax.fori_loop(0, n, turn, 0)

    gap = 1.0 - bound_ref[...]
    row = lax.broadcasted_iota(jnp.int32, (length, length), 0)
    col = lax.broadcasted_iota(jnp.int32, (length, length), 1)
    causal = row >= col
    ones = causal.astype(jnp.bfloat16)
    ones = jnp.concatenate([ones, ones], axis=1)
    middle = length // 2

    def seq_rows(s):
        return pl.ds(pl.multiple_of(s * length, length), length)

    def project(u, dest, at, tiles):
        def step(j, carry):
            lanes = pl.ds(pl.multiple_of(j * half, half), half)
            there = pl.ds(pl.multiple_of(at + j * half, half), half)
            dest[:, there] = jnp.dot(
                normed[...], wholes[u][:, lanes], preferred_element_type=jnp.float32
            ).astype(jnp.bfloat16)
            return carry

        lax.fori_loop(0, tiles, step, 0)

    def decays(g, s):
        rows = seq_rows(s)
        lanes = slice(g * half, (g + 1) * half)
        keys = gap[:, lanes] * jax.nn.sigmoid(-f_ref[rows, lanes].astype(jnp.float32))
        spread = jnp.concatenate(
            [
                jnp.broadcast_to(
                    extra_ref[s * (heads // own) + h // own][:length, h % own : h % own + 1],
                    (length, hk),
                )
                for h in (2 * g, 2 * g + 1)
            ],
            axis=1,
        )
        decay = jnp.log(1.0 - keys) + spread
        high = decay.astype(jnp.bfloat16)
        low = (decay - high.astype(jnp.float32)).astype(jnp.bfloat16)
        cum = jnp.dot(
            ones, jnp.concatenate([high, low], axis=0), preferred_element_type=jnp.float32
        )
        mid = cum[middle : middle + 1, :]
        end = cum[length - 1 : length, :]
        rel = cum - mid
        keys_ref[rows, lanes] = (keys * jnp.exp(-rel)).astype(jnp.bfloat16)
        rel_ref[rows, lanes] = rel
        emid_ref[pl.ds(s, 1), lanes] = jnp.exp(mid)
        eend_ref[pl.ds(s, 1), lanes] = jnp.exp(end - mid)
        both = jnp.exp(end)
        mine = jnp.where(side == 0, both[:, :hk], both[:, hk:])
        other = jnp.where(side == 0, both[:, hk:], both[:, :hk])
        dbuf[side, g, pl.ds(s, 1)] = mine
        dsend[g, pl.ds(s, 1)] = other

    def head_lanes(g, role):
        start = g * half + (side if role == 0 else 1 - side) * hk
        return pl.ds(pl.multiple_of(start, hk), hk)

    def added(g, s, role):
        rows = seq_rows(s)
        lanes = head_lanes(g, role)
        state = lax.dot_general(
            v_ref[rows, lanes], keys_ref[rows, lanes], TN, preferred_element_type=jnp.float32
        )
        ends = eend_ref[pl.ds(s, 1), g * half : (g + 1) * half]
        end = jnp.where(side == role, ends[:, :hk], ends[:, hk:])
        return (state * end).astype(jnp.bfloat16)

    def locals_of(g, s):
        k = g * seqs + s
        bs[k] = added(g, s, 1)
        b_copy(k).start()
        bb[k, side] = added(g, s, 0)

    def chain(k, carry):
        g = k // seqs
        s = lax.rem(k, seqs)
        holder = (s * heads + 2 * g + side) // own
        b_copy(k).wait_recv()

        @pl.when(jnp.logical_or(level > 0, holder != me))
        def _():
            c_copy(k).wait_recv()

        first = dbuf[0, g, pl.ds(s, 1)]
        between = st[k, 0].astype(jnp.float32) * first + bb[k, 0].astype(jnp.float32)
        st[k, 1] = between.astype(jnp.bfloat16)
        t_copy(k).start()

        @pl.when(level < levels - 1)
        def _():
            second = dbuf[1, g, pl.ds(s, 1)]
            ob[k] = (between * second + bb[k, 1].astype(jnp.float32)).astype(jnp.bfloat16)
            c_copy(k).start()

        return carry

    lag = 4

    def target(i):
        late = i + 1 - lag * level
        first = jnp.clip(late, 0, seqs)
        later = jnp.clip(late - 2 * seqs, 0, total - seqs)
        return first + later

    def chain_slot(i):
        lax.fori_loop(target(i - 1), target(i), chain, 0)

    def intra(s):
        rows = seq_rows(s)
        q_pre = q_ref[rows, :].astype(jnp.float32)
        q_mid = q_pre * jax.nn.sigmoid(q_pre) * jnp.exp(rel_ref[rows, :])
        q_near = q_mid.astype(jnp.bfloat16)
        q_ref[rows, :] = (q_mid * emid_ref[pl.ds(s, 1), :]).astype(jnp.bfloat16)
        for h in range(heads):
            lanes = slice(h * hk, (h + 1) * hk)
            scores = lax.dot_general(
                q_near[:, lanes], keys_ref[rows, lanes], NT, preferred_element_type=jnp.float32
            )
            scores = jnp.where(causal, scores, 0.0).astype(jnp.bfloat16)
            within_ref[rows, lanes] = jnp.dot(
                scores, v_ref[rows, lanes], preferred_element_type=jnp.float32
            )

    def finish(t, carry):
        for b in range(2):
            s = 2 * t + b
            rows = seq_rows(s)
            for g in range(groups):
                k = g * seqs + s
                for role in range(2):
                    lanes = head_lanes(g, role)
                    state = st[k, side] if role == 0 else fin[k]
                    outs = within_ref[rows, lanes] + lax.dot_general(
                        q_ref[rows, lanes], state, NT, preferred_element_type=jnp.float32
                    )
                    scaled = rms_scale(outs, gain_ref[...]).astype(jnp.bfloat16)
                    g_pre = g_ref[rows, lanes].astype(jnp.float32)
                    gated_ref[b * length : (b + 1) * length, lanes] = (
                        scaled.astype(jnp.float32) * (g_pre * jax.nn.sigmoid(g_pre))
                    ).astype(jnp.bfloat16)
        tile = 512
        squares = jnp.zeros((2 * length, 1), jnp.float32)
        for j in range(width // tile):
            lanes = slice(j * tile, (j + 1) * tile)
            mixed = jnp.dot(
                gated_ref[...], wholes[unit_o][:, lanes], preferred_element_type=jnp.float32
            )
            squares = squares + jnp.sum(mixed * mixed, axis=-1, keepdims=True)
            mixed_ref[:, lanes] = mixed
        scale = lax.rsqrt(squares * (1.0 / width) + EPS)
        rows = pl.ds(pl.multiple_of(t * 2 * length, 2 * length), 2 * length)
        for j in range(width // tile):
            lanes = slice(j * tile, (j + 1) * tile)
            out_ref[rows, lanes] = (mixed_ref[:, lanes] * scale * post_ref[:, lanes]).astype(
                jnp.bfloat16
            )
        return carry

    pass_y(0)
    pass_y(1)
    pass_r(0)
    arrived(0)
    project(0, f_ref, 0, 1)
    pass_y(2)

    def decay_first(s, carry):
        decays(0, s)

        @pl.when(s == seqs // 2)
        def _():
            pass_r(1)

        return carry

    lax.fori_loop(0, seqs, decay_first, 0)
    d_copy(0).start()
    pass_y(3)
    arrived(1)
    project(1, v_ref, 0, 1)

    def locals_first(s, carry):
        locals_of(0, s)
        return carry

    lax.fori_loop(0, seqs, locals_first, 0)
    pass_r(2)
    arrived(2)
    project(2, f_ref, half, 1)
    d_copy(0).wait_recv()

    def decay_later(s, carry):
        decays(1, s)
        chain_slot(s)

        @pl.when(s == seqs // 4)
        def _():
            pass_r(3)

        @pl.when(s == seqs // 2)
        def _():
            pass_y(unit_q)

        return carry

    lax.fori_loop(0, seqs, decay_later, 0)
    d_copy(1).start()
    arrived(3)
    project(3, v_ref, half, 1)

    def locals_later(s, carry):
        locals_of(1, s)
        chain_slot(seqs + s)

        @pl.when(s == seqs // 2)
        def _():
            pass_r(unit_q)

        return carry

    lax.fori_loop(0, seqs, locals_later, 0)
    pass_y(unit_g)
    d_copy(1).wait_recv()
    arrived(unit_q)
    project(unit_q, q_ref, 0, cols // half)

    def intra_later(s, carry):
        intra(s)
        chain_slot(2 * seqs + s)

        @pl.when(s == seqs // 2)
        def _():
            pass_r(unit_g)

        return carry

    lax.fori_loop(0, seqs, intra_later, 0)
    pass_y(unit_o)
    arrived(unit_g)
    project(unit_g, g_ref, 0, cols // half)
    arrived(unit_o)

    def ending(t, carry):
        done = target(3 * seqs - 1)

        def goal(t):
            return jnp.maximum(jnp.minimum(total - seqs + 2 * t + 4, total), done)

        before = jnp.where(t == 0, done, goal(t - 1))
        lax.fori_loop(before, goal(t), chain, 0)
        for g in range(groups):
            for b in range(2):
                t_copy(g * seqs + 2 * t + b).wait_recv()
        return finish(t, carry)

    lax.fori_loop(0, seqs // 2, ending, 0)

    for offset in range(1, n):
        e_copy(offset).wait_send()
    for j in range(own):
        holder_target, _ = place(j)

        @pl.when(me != holder_target)
        def _():
            i_copy(j).wait_send()

    for u in range(units):
        s_own(u).wait_send()
        for k in range(peers):
            y_copy(u, k).wait_send()
            s_copy(u, k, 0).wait_send()
            if axes[u] is not None:
                r_copy(u, k).wait_send()
                s_copy(u, k, 1).wait_send()
    for g in range(groups):
        d_copy(g).wait_send()

    def drain(k, carry):
        b_copy(k).wait_send()
        t_copy(k).wait_send()

        @pl.when(level < levels - 1)
        def _():
            c_copy(k).wait_send()

        return carry

    lax.fori_loop(0, total, drain, 0)


def body(
    n,
    ways,
    tokens,
    pre_gain,
    w_query,
    w_forget,
    w_value,
    w_gate,
    lower_bound,
    extra_decay,
    initial_state,
    norm_gain,
    w_out,
    post_gain,
):
    seqs, length, width = tokens.shape
    own, hk, hv = initial_state.shape
    items = own * n
    heads = items // seqs
    groups = heads // 2
    half = 2 * hk
    cols = heads * hk
    rows = seqs * length
    total = groups * seqs
    peers = max(ways // 2 - 1, 1)
    axes = ("x", "x") + ("z", "z") * (groups - 1) + ("z", "z", None)
    units = len(axes)
    dma = pltpu.SemaphoreType.DMA
    bf16, f32 = jnp.bfloat16, jnp.float32
    small = (
        pre_gain[None, :],
        lower_bound[None, :],
        norm_gain[None, :],
        post_gain[None, :],
    )
    shapes = [(width, half)] * (2 * groups) + [(width, cols)] * 2 + [(cols, width)]
    out = pl.pallas_call(
        functools.partial(layer_kernel, n, ways, heads, axes),
        out_shape=jax.ShapeDtypeStruct((rows, width), bf16),
        in_specs=[pl.BlockSpec(memory_space=pltpu.HBM)] * 12,
        out_specs=pl.BlockSpec(memory_space=pltpu.VMEM),
        scratch_shapes=[pltpu.VMEM(shape, bf16) for shape in shapes]
        + [
            pltpu.VMEM(tokens.shape, bf16),
            pltpu.VMEM((1, width), f32),
            pltpu.VMEM(extra_decay.shape, f32),
            pltpu.VMEM((1, cols), f32),
            pltpu.VMEM(initial_state.shape, f32),
            pltpu.VMEM((1, hv), f32),
            pltpu.VMEM((1, width), f32),
            pltpu.VMEM((rows, width), bf16),
            pltpu.VMEM((rows, cols), bf16),
            pltpu.VMEM((rows, cols), bf16),
            pltpu.VMEM((rows, cols), bf16),
            pltpu.VMEM((rows, cols), bf16),
            pltpu.VMEM((rows, cols), bf16),
            pltpu.VMEM((rows, cols), f32),
            pltpu.VMEM((seqs, cols), f32),
            pltpu.VMEM((seqs, cols), f32),
            pltpu.VMEM((rows, cols), f32),
            pltpu.VMEM((2 * length, cols), bf16),
            pltpu.VMEM((2 * length, width), f32),
            pltpu.VMEM((n, own, 128), f32),
            pltpu.VMEM((n, own, 128), f32),
            pltpu.VMEM((n, 128, own), f32),
            pltpu.VMEM((own, hv, hk), bf16),
            pltpu.VMEM((total, 2, hv, hk), bf16),
            pltpu.VMEM((total, hv, hk), bf16),
            pltpu.VMEM((total, 2, hv, hk), bf16),
            pltpu.VMEM((total, hv, hk), bf16),
            pltpu.VMEM((total, hv, hk), bf16),
            pltpu.VMEM((2, groups, seqs, hk), f32),
            pltpu.VMEM((groups, seqs, hk), f32),
            dma((units + 7,)),
            dma((units, peers)),
            dma((units, peers)),
            dma((units, peers)),
            dma((units, peers)),
            dma((units, 1 + 2 * peers)),
            dma((units, 1 + 2 * peers)),
            dma((n - 1,)),
            dma((n - 1,)),
            dma((own,)),
            dma((total,)),
            dma((total,)),
            dma((groups,)),
            dma((groups,)),
            dma((total,)),
            dma((total,)),
            dma((total,)),
            dma((total,)),
        ],
        compiler_params=pltpu.CompilerParams(
            collective_id=0, has_side_effects=True, vmem_limit_bytes=67043328 - rows * width * 2
        ),
        cost_estimate=pl.CostEstimate(
            flops=6 * 10**9, bytes_accessed=2 * 10**7, transcendentals=10**6
        ),
    )(
        tokens,
        small[0],
        w_forget,
        w_value,
        w_query,
        w_gate,
        w_out,
        extra_decay,
        small[1],
        initial_state,
        small[2],
        small[3],
    )
    return out.reshape(seqs, length, width)


def solution(mesh):
    in_specs = (
        P("dp", "sp", None),
        P(),
        P("dp", None),
        P("dp", None),
        P("dp", None),
        P("dp", None),
        P(),
        P(("dp", "sp"), None),
        P(("dp", "sp"), None, None),
        P(),
        P("dp", None),
        P(),
    )
    out_specs = P("dp", "sp", None)
    return jax.shard_map(
        functools.partial(body, mesh.shape["sp"], mesh.shape["dp"]),
        mesh=mesh,
        in_specs=in_specs,
        out_specs=out_specs,
        check_vma=False,
    )
```

```python
import functools

import jax
import jax.numpy as jnp
from jax import lax
from jax.experimental import pallas as pl
from jax.experimental.pallas import tpu as pltpu
from jax.sharding import PartitionSpec as P

EPS = 1e-06
MESH = pl.DeviceIdType.MESH
NT = (((1,), (1,)), ((), ()))
TN = (((0,), (0,)), ((), ()))


def rms_scale(matrix, gain):
    widened = matrix.astype(jnp.float32)
    return widened * lax.rsqrt(jnp.mean(widened * widened, axis=-1, keepdims=True) + EPS) * gain


def layer_kernel(
    n,
    ways,
    heads,
    axes,
    tokens_hbm,
    pre_hbm,
    wf_hbm,
    wv_hbm,
    wq_hbm,
    wg_hbm,
    wo_hbm,
    extra_hbm,
    bound_hbm,
    init_hbm,
    gain_hbm,
    out_ref,
    *scratch,
):
    units = len(axes)
    groups = heads // 2
    wholes = scratch[:units]
    (
        tokens_ref,
        pre_ref,
        raw_ref,
        bound_ref,
        start_ref,
        gain_ref,
        normed,
        f_ref,
        v_ref,
        q_ref,
        g_ref,
        keys_ref,
        rel_ref,
        gap_ref,
        emid_ref,
        eend_ref,
        within_ref,
        gated_ref,
        esend,
        erecv,
        extra_ref,
        isend,
        st,
        fin,
        bb,
        bs,
        ob,
        dbuf,
        dsend,
        local_sem,
        y_send,
        y_recv,
        r_send,
        r_recv,
        s_send,
        s_recv,
        e_send,
        e_recv,
        i_send,
        b_send,
        b_recv,
        d_send,
        d_recv,
        c_send,
        c_recv,
        t_send,
        t_recv,
        up_sem,
        down_sem,
    ) = scratch[units:]
    me = lax.axis_index("sp")
    rank = lax.axis_index("dp")
    seqs, length, width = tokens_ref.shape
    own, hk, hv = start_ref.shape
    half = 2 * hk
    total = groups * seqs
    levels = n // 2
    side = lax.rem(me, 2)
    level = me // 2
    parity = lax.rem(level, 2)
    beside = me + 1 - 2 * side
    above = lax.rem(me + 2, n)
    below = lax.rem(me + n - 2, n)
    sibling = rank + 1 - 2 * lax.rem(rank, 2)
    peers = ways // 2 - 1
    not_top = level < levels - 1
    not_base = level > 0
    second_top = level == levels - 2
    unit_f = 4
    unit_q = unit_f + 2 * (groups - 1)
    unit_g = unit_q + groups
    unit_o = unit_g + groups

    def group_cols(base, g):
        return base.at[:, g * half : (g + 1) * half]

    def source(u):
        if u < 4:
            base = wf_hbm if u % 2 == 0 else wv_hbm
            head = side if u >= 2 else 1 - side
            return base.at[:, pl.ds(pl.multiple_of(head * hk, hk), hk)]
        if u < unit_q:
            return group_cols(wf_hbm if u % 2 == 0 else wv_hbm, (u - unit_f) // 2 + 1)
        if u < unit_g:
            return group_cols(wq_hbm, u - unit_q)
        if u < unit_o:
            return group_cols(wg_hbm, u - unit_g)
        part = width // 2
        return wo_hbm.at[:, (u - unit_o) * part : (u - unit_o + 1) * part]

    def full(u, shard):
        rows = wholes[u].shape[0] // ways
        return wholes[u].at[pl.ds(pl.multiple_of(shard * rows, rows), rows)]

    def part(u, shard, which):
        rows = wholes[u].shape[0] // ways
        start = shard * rows + which * (rows // 2)
        return wholes[u].at[pl.ds(pl.multiple_of(start, rows // 2), rows // 2)]

    def local_copy(u):
        return pltpu.make_async_copy(source(u), full(u, rank), local_sem.at[min(u, 2)])

    small = [
        pltpu.make_async_copy(src, dst, local_sem.at[3 + j])
        for j, (src, dst) in enumerate(
            (
                (tokens_hbm, tokens_ref),
                (pre_hbm, pre_ref),
                (extra_hbm, raw_ref),
                (init_hbm, start_ref),
                (bound_hbm, bound_ref),
                (gain_hbm, gain_ref),
            )
        )
    ]
    for u in (0, 1):
        local_copy(u).start()
    small[0].start()
    small[1].start()
    for u in range(2, units):
        local_copy(u).start()
    for copy in small[2:]:
        copy.start()

    barrier = pltpu.get_barrier_semaphore()

    def greet(device):
        pl.semaphore_signal(barrier, inc=1, device_id=device, device_id_type=MESH)

    greet({"sp": beside})
    for offset in range(1, ways):
        greet({"dp": lax.rem(rank + offset, ways)})

    @pl.when(not_top)
    def _():
        greet({"sp": above})

    @pl.when(not_base)
    def _():
        greet({"sp": below})

    pl.semaphore_wait(
        barrier, ways + not_top.astype(jnp.int32) + not_base.astype(jnp.int32)
    )

    def remote(src, dst, send, recv, device):
        return pltpu.make_async_remote_copy(
            src_ref=src,
            dst_ref=dst,
            send_sem=send,
            recv_sem=recv,
            device_id=device,
            device_id_type=MESH,
        )

    def settle(sem, rows, ref=None):
        ref = out_ref if ref is None else ref
        if rows:
            view = ref.at[0:rows]
            pltpu.make_async_copy(view, view, sem).wait()

    def bulk(us, halves=False):
        line = width * 4
        size = sum(wholes[u].shape[0] // ways * wholes[u].shape[1] * 2 for u in us)
        return size // (2 if halves else 1) // line

    z_units = [u for u in range(units) if axes[u] == "z"]

    def first_part(u, shard):
        return part(u, shard, parity) if axes[u] == "z" else full(u, shard)

    def y_copy(u, k):
        ref = first_part(u, rank)
        target = lax.rem(rank + 2 * (k + 1), ways)
        return remote(ref, ref, y_send.at[k], y_recv.at[u, k], {"dp": target})

    def origin(k):
        return lax.rem(rank + ways - 2 * (k + 1), ways)

    def m_copy(u, k):
        src, dst = full(u, origin(k)), full(u + 2, origin(k))
        return remote(src, dst, r_send.at[0, k], r_recv.at[u + 2, k], {"sp": beside})

    def z_copy(u, k, upward):
        ref = part(u, origin(k), parity)
        device = {"sp": above if upward else below}
        return remote(ref, ref, r_send.at[1 + upward, k], r_recv.at[u, k], device)

    def relay(u, k):
        if axes[u] == "y":
            m_copy(u, k).start()
        if axes[u] == "z":

            @pl.when(not_base)
            def _():
                z_copy(u, k, 0).start()

            @pl.when(second_top)
            def _():
                z_copy(u, k, 1).start()

    def s_own(u):
        ref = full(u, rank)
        return remote(ref, ref, s_send.at[0], s_recv.at[u], {"dp": sibling})

    def s_copy(u, k, second):
        ref = part(u, origin(k), 1 - parity) if second else first_part(u, origin(k))
        return remote(ref, ref, s_send.at[1 + k], s_recv.at[u], {"dp": sibling})

    def pass_y(u):
        for k in range(peers):
            y_copy(u, k).wait_recv()
            relay(u, k)
            s_copy(u, k, 0).start()

    def pass_r(u):
        for k in range(peers):
            if axes[u] == "m":
                m_copy(u - 2, k).wait_recv()
                s_copy(u, k, 0).start()
            else:
                z_copy(u, k, 0).wait_recv()
                s_copy(u, k, 1).start()

    def arrived(u):
        settle(s_recv.at[u], wholes[u].shape[0] // 2, wholes[u])

    def e_copy(offset):
        target = lax.rem(me + offset, n)
        return remote(
            esend.at[target],
            erecv.at[me],
            e_send,
            e_recv.at[offset - 1],
            {"sp": target},
        )

    near = jnp.where(side == 0, 1, n - 1)

    def place(j):
        it = me * own + j
        h = lax.rem(it, heads)
        return lax.rem(h, 2), (h // 2) * seqs + it // heads

    def i_copy(j):
        target, k = place(j)
        return remote(isend.at[j], st.at[k, 0], i_send.at[j], c_recv.at[k], {"sp": target})

    def b_copy(k):
        return remote(bs.at[k], bb.at[k, side], b_send, b_recv.at[k], {"sp": beside})

    def d_copy(g):
        return remote(dsend.at[g], dbuf.at[side, g], d_send, d_recv.at[g], {"sp": beside})

    def c_copy(k):
        return remote(ob.at[k], st.at[k, 0], c_send, c_recv.at[k], {"sp": above})

    def t_copy(k):
        return remote(st.at[k, 1 - side], fin.at[k], t_send, t_recv.at[k], {"sp": beside})

    for u in range(units):
        if u < 2:
            local_copy(u).wait()
        if u == 2:
            settle(local_sem.at[2], bulk(range(2, units)))
        if axes[u] != "m":
            for k in range(peers):
                y_copy(u, k).start()
        s_own(u).start()

    def tell(sem, device):
        pl.semaphore_signal(sem, inc=1, device_id={"sp": device}, device_id_type=MESH)

    @pl.when(jnp.logical_not(not_base))
    def _():
        tell(up_sem, above)

    @pl.when(jnp.logical_not(not_top))
    def _():
        tell(down_sem, below)

    @pl.when(not_base)
    def _():
        pl.semaphore_wait(up_sem, 1)

        @pl.when(not_top)
        def _():
            tell(up_sem, above)
            pl.semaphore_wait(down_sem, 1)
            tell(down_sem, below)

    for copy in small:
        copy.wait()

    def norm_rows(s, carry):
        rows = pl.ds(pl.multiple_of(s * length, length), length)
        normed[rows, :] = rms_scale(tokens_ref[s], pre_ref[...]).astype(jnp.bfloat16)
        return carry

    def send_extras():
        for offset in range(1, n):

            @pl.when(offset != near)
            def _():
                e_copy(offset).start()

    def send_states():
        for j in range(own):
            target, k = place(j)

            @pl.when(me != target)
            def _():
                i_copy(j).start()

            @pl.when(me == target)
            def _():
                st[k, 0] = isend[j]

    pad = esend.shape[2]
    for p in range(n):
        piece = raw_ref[:, p * length : (p + 1) * length]
        esend[p] = jnp.concatenate(
            [piece, jnp.zeros((own, pad - length), jnp.float32)], axis=1
        )
    e_copy(near).start()

    @pl.when(not_base)
    def _():
        send_extras()

    for j in range(own):
        isend[j] = start_ref[j].T.astype(jnp.bfloat16)
    for h in range(heads):
        gap_ref[h] = 1.0 - bound_ref[:, h * hk : (h + 1) * hk]
    erecv[me] = esend[me]

    lax.fori_loop(0, seqs, norm_rows, 0)

    @pl.when(level < 2)
    def _():
        send_states()

    pass_y(0)

    @pl.when(jnp.logical_not(not_base))
    def _():
        pl.semaphore_wait(down_sem, 1)
        send_extras()

    row = lax.broadcasted_iota(jnp.int32, (length, length), 0)
    col = lax.broadcasted_iota(jnp.int32, (length, length), 1)
    causal = row >= col
    ones = causal.astype(jnp.bfloat16)
    ones = jnp.concatenate([ones, ones], axis=1)
    middle = length // 2

    def seq_rows(s):
        return pl.ds(pl.multiple_of(s * length, length), length)

    def head_of(g, role):
        return 2 * g + (side if role == 0 else 1 - side)

    def head_lanes(g, role):
        return pl.ds(pl.multiple_of(head_of(g, role) * hk, hk), hk)

    def project(u, dest, lanes):
        dest[:, lanes] = jnp.dot(
            normed[...], wholes[u][...], preferred_element_type=jnp.float32
        ).astype(jnp.bfloat16)

    def group_lanes(g):
        return slice(g * half, (g + 1) * half)

    def extras(s):
        for j in range(heads // own):
            p = s * (heads // own) + j
            offset = lax.rem(me - p + n, n)

            @pl.when(offset > 0)
            def _():
                e_copy(offset).wait_recv()

            extra_ref[p] = erecv[p].T

    def decays(g, role, s):
        rows = seq_rows(s)
        lanes = head_lanes(g, role)
        head = head_of(g, role)
        keys = gap_ref[head] * jax.nn.sigmoid(-f_ref[rows, lanes].astype(jnp.float32))
        columns = [
            extra_ref[s * (heads // own) + h // own][:length, h % own : h % own + 1]
            for h in (2 * g, 2 * g + 1)
        ]
        spread = jnp.where(side == role, columns[0], columns[1])
        decay = jnp.log(1.0 - keys) + spread
        high = decay.astype(jnp.bfloat16)
        low = (decay - high.astype(jnp.float32)).astype(jnp.bfloat16)
        cum = jnp.dot(
            ones, jnp.concatenate([high, low], axis=0), preferred_element_type=jnp.float32
        )
        mid = cum[middle : middle + 1, :]
        end = cum[length - 1 : length, :]
        rel = cum - mid
        keys_ref[rows, lanes] = (keys * jnp.exp(-rel)).astype(jnp.bfloat16)
        rel_ref[rows, lanes] = rel
        emid_ref[head, pl.ds(s, 1)] = jnp.exp(mid)
        eend_ref[head, pl.ds(s, 1)] = jnp.exp(end - mid)
        if role == 0:
            dbuf[side, g, pl.ds(s, 1)] = jnp.exp(end)
        else:
            dsend[g, pl.ds(s, 1)] = jnp.exp(end)

    def added(g, role, s):
        rows = seq_rows(s)
        lanes = head_lanes(g, role)
        state = lax.dot_general(
            v_ref[rows, lanes], keys_ref[rows, lanes], TN, preferred_element_type=jnp.float32
        )
        return (state * eend_ref[head_of(g, role), pl.ds(s, 1)]).astype(jnp.bfloat16)

    def local_sent(g, s):
        k = g * seqs + s
        bs[k] = added(g, 1, s)
        b_copy(k).start()

    def local_kept(g, s):
        bb[g * seqs + s, side] = added(g, 0, s)

    def chain(k, carry):
        g = k // seqs
        s = lax.rem(k, seqs)
        holder = (s * heads + 2 * g + side) // own
        b_copy(k).wait_recv()

        @pl.when(jnp.logical_or(not_base, holder != me))
        def _():
            c_copy(k).wait_recv()

        first = dbuf[0, g, pl.ds(s, 1)]
        between = st[k, 0].astype(jnp.float32) * first + bb[k, 0].astype(jnp.float32)
        st[k, 1] = between.astype(jnp.bfloat16)
        t_copy(k).start()

        @pl.when(not_top)
        def _():
            second = dbuf[1, g, pl.ds(s, 1)]
            ob[k] = (between * second + bb[k, 1].astype(jnp.float32)).astype(jnp.bfloat16)
            c_copy(k).start()

        return carry

    def reached(g, time):
        begin = 182 + 93 * g + jnp.where(not_base, 14 + 18 * level, 0)
        return g * seqs + jnp.clip(time - begin + 7, 0, 7 * seqs) // 7

    def advance(before, now):
        for g in range(groups):
            lax.fori_loop(reached(g, before), reached(g, now), chain, 0)

    def intra(s):
        rows = seq_rows(s)
        for h in range(heads):
            lanes = slice(h * hk, (h + 1) * hk)
            q_pre = q_ref[rows, lanes].astype(jnp.float32)
            q_mid = q_pre * jax.nn.sigmoid(q_pre) * jnp.exp(rel_ref[rows, lanes])
            q_ref[rows, lanes] = (q_mid * emid_ref[h, pl.ds(s, 1)]).astype(jnp.bfloat16)
            scores = lax.dot_general(
                q_mid.astype(jnp.bfloat16),
                keys_ref[rows, lanes],
                NT,
                preferred_element_type=jnp.float32,
            )
            scores = jnp.where(causal, scores, 0.0).astype(jnp.bfloat16)
            within_ref[rows, lanes] = jnp.dot(
                scores, v_ref[rows, lanes], preferred_element_type=jnp.float32
            )

    def finish(t, carry):
        for b in range(2):
            s = 2 * t + b
            rows = seq_rows(s)
            for g in range(groups):
                k = g * seqs + s
                for role in range(2):
                    lanes = head_lanes(g, role)
                    state = st[k, side] if role == 0 else fin[k]
                    outs = within_ref[rows, lanes] + lax.dot_general(
                        q_ref[rows, lanes], state, NT, preferred_element_type=jnp.float32
                    )
                    scaled = rms_scale(outs, gain_ref[...]).astype(jnp.bfloat16)
                    g_pre = g_ref[rows, lanes].astype(jnp.float32)
                    gated_ref[b * length : (b + 1) * length, lanes] = (
                        scaled.astype(jnp.float32) * (g_pre * jax.nn.sigmoid(g_pre))
                    ).astype(jnp.bfloat16)
        tile = 512
        squares = jnp.zeros((2 * length, 1), jnp.float32)
        rows = pl.ds(pl.multiple_of(t * 2 * length, 2 * length), 2 * length)
        tiles = [
            (unit_o + p, slice(j * tile, (j + 1) * tile), p * (width // 2) + j * tile)
            for p in range(2)
            for j in range(width // 2 // tile)
        ]
        for u, lanes, at in tiles:
            mixed = jnp.dot(
                gated_ref[...], wholes[u][:, lanes], preferred_element_type=jnp.float32
            )
            squares = squares + jnp.sum(mixed * mixed, axis=-1, keepdims=True)
            out_ref[rows, at : at + tile] = mixed
        scale = lax.rsqrt(squares * (1.0 / width) + EPS)
        for u, lanes, at in tiles:
            out_ref[rows, at : at + tile] = out_ref[rows, at : at + tile] * scale
        return carry

    def loop(step, hooks=(), count=seqs):
        def run(s, carry):
            step(s)
            for at, act in hooks:

                @pl.when(s == at)
                def _():
                    act()

            return carry

        lax.fori_loop(0, count, run, 0)

    def paired(step):
        def run(t):
            step(2 * t)
            step(2 * t + 1)

        return run

    twos = seqs // 2
    arrived(0)
    project(0, f_ref, head_lanes(0, 1))
    pass_y(1)

    def first_decays(t):
        for s in (2 * t, 2 * t + 1):
            extras(s)
        for s in (2 * t, 2 * t + 1):
            decays(0, 1, s)

    loop(first_decays, count=twos)
    d_copy(0).start()
    arrived(1)
    project(1, v_ref, head_lanes(0, 1))
    pass_y(4)

    @pl.when(level >= 2)
    def _():
        send_states()

    loop(paired(lambda s: local_sent(0, s)), count=twos)
    pass_r(2)
    arrived(2)
    project(2, f_ref, head_lanes(0, 0))
    loop(paired(lambda s: decays(0, 0, s)), ((twos - 1, lambda: pass_r(3)),), count=twos)
    pass_y(5)
    arrived(3)
    project(3, v_ref, head_lanes(0, 0))
    d_copy(0).wait_recv()
    loop(paired(lambda s: local_kept(0, s)), count=twos)
    pass_r(4)
    pass_y(6)
    arrived(4)
    project(4, f_ref, group_lanes(1))
    advance(0, 205)

    def later_other(t):
        decays(1, 1, 2 * t)
        decays(1, 1, 2 * t + 1)
        advance(205 + 3 * t, 208 + 3 * t)

    def later_mine(t):
        decays(1, 0, 2 * t)
        decays(1, 0, 2 * t + 1)
        advance(239 + 3 * t, 242 + 3 * t)

    def later_sent(t):
        local_sent(1, 2 * t)
        local_sent(1, 2 * t + 1)
        advance(227 + 3 * t, 230 + 3 * t)

    def later_kept(t):
        local_kept(1, 2 * t)
        local_kept(1, 2 * t + 1)
        advance(251 + 3 * t, 254 + 3 * t)

    loop(later_other, count=twos)
    d_copy(1).start()
    pass_r(5)
    pass_y(7)
    arrived(5)
    project(5, v_ref, group_lanes(1))
    advance(205 + 3 * twos, 227)
    pass_y(8)
    loop(later_sent, count=twos)
    loop(later_mine, count=twos)
    pass_y(9)
    pass_r(6)
    loop(later_kept, count=twos)
    pass_y(10)
    d_copy(1).wait_recv()
    time = 251 + 3 * twos
    pass_r(7)
    arrived(6)
    project(6, q_ref, group_lanes(0))
    advance(time, 275)
    arrived(7)
    project(7, q_ref, group_lanes(1))
    advance(275, 293)
    pass_r(8)
    pass_y(11)

    def intra_slot(s):
        intra(s)
        advance(293 + 6 * s, 299 + 6 * s)

    loop(
        intra_slot,
        (
            (seqs // 2, lambda: pass_r(9)),
            (seqs - 2, lambda: pass_r(10)),
        ),
    )
    time = 293 + 6 * seqs
    arrived(8)
    project(8, g_ref, group_lanes(0))
    advance(time, 356)
    arrived(9)
    project(9, g_ref, group_lanes(1))
    advance(356, 368)
    lax.fori_loop(reached(0, 368), seqs, chain, 0)
    done = jnp.where(not_top, total, reached(1, 368))
    lax.fori_loop(reached(1, 368), done, chain, 0)
    pass_r(11)

    settle(e_send, n - 1, esend)
    for j in range(own):
        holder_target, _ = place(j)

        @pl.when(me != holder_target)
        def _():
            i_copy(j).wait_send()

    settle(d_send, groups, dsend)
    settle(b_send, total, bs)
    settle(s_send.at[0], bulk(range(units)))
    for k in range(peers):
        settle(y_send.at[k], bulk((0, 1)) + bulk(z_units, True))
        settle(r_send.at[0, k], bulk((0, 1)))
        settle(s_send.at[1 + k], bulk(range(units)))

        @pl.when(not_base)
        def _():
            settle(r_send.at[1, k], bulk(z_units, True))

        @pl.when(second_top)
        def _():
            settle(r_send.at[2, k], bulk(z_units, True))

    arrived(10)
    arrived(11)

    def ending(t, carry):
        def goal(t):
            return jnp.maximum(seqs + jnp.minimum(2 * t + 4, seqs), done)

        lax.fori_loop(jnp.where(t == 0, done, goal(t - 1)), goal(t), chain, 0)
        for g in range(groups):
            for b in range(2):
                t_copy(g * seqs + 2 * t + b).wait_recv()
        return finish(t, carry)

    lax.fori_loop(0, seqs // 2, ending, 0)

    settle(t_send, total, fin)

    @pl.when(not_top)
    def _():
        settle(c_send, total, ob)


def body(
    n,
    ways,
    tokens,
    pre_gain,
    w_query,
    w_forget,
    w_value,
    w_gate,
    lower_bound,
    extra_decay,
    initial_state,
    norm_gain,
    w_out,
    post_gain,
):
    seqs, length, width = tokens.shape
    own, hk, hv = initial_state.shape
    items = own * n
    heads = items // seqs
    groups = heads // 2
    half = 2 * hk
    cols = heads * hk
    rows = seqs * length
    total = groups * seqs
    peers = max(ways // 2 - 1, 1)
    axes = ("y", "y", "m", "m") + ("z",) * (2 * (groups - 1) + 2 * groups + 2)
    units = len(axes)
    dma = pltpu.SemaphoreType.DMA
    bf16, f32 = jnp.bfloat16, jnp.float32
    shapes = [(width, hk)] * 4 + [(width, half)] * (4 * groups - 2) + [(cols, width // 2)] * 2
    out = pl.pallas_call(
        functools.partial(layer_kernel, n, ways, heads, axes),
        out_shape=pltpu.VMEM((rows, width), f32),
        in_specs=[pl.BlockSpec(memory_space=pltpu.HBM)] * 11,
        out_specs=pl.BlockSpec(memory_space=pltpu.VMEM),
        scratch_shapes=[pltpu.VMEM(shape, bf16) for shape in shapes]
        + [
            pltpu.VMEM(tokens.shape, bf16),
            pltpu.VMEM((1, width), f32),
            pltpu.VMEM(extra_decay.shape, f32),
            pltpu.VMEM((1, cols), f32),
            pltpu.VMEM(initial_state.shape, f32),
            pltpu.VMEM((1, hv), f32),
            pltpu.VMEM((rows, width), bf16),
            pltpu.VMEM((rows, cols), bf16),
            pltpu.VMEM((rows, cols), bf16),
            pltpu.VMEM((rows, cols), bf16),
            pltpu.VMEM((rows, cols), bf16),
            pltpu.VMEM((rows, cols), bf16),
            pltpu.VMEM((rows, cols), f32),
            pltpu.VMEM((heads, 1, hk), f32),
            pltpu.VMEM((heads, seqs, hk), f32),
            pltpu.VMEM((heads, seqs, hk), f32),
            pltpu.VMEM((rows, cols), f32),
            pltpu.VMEM((2 * length, cols), bf16),
            pltpu.VMEM((n, own, 128), f32),
            pltpu.VMEM((n, own, 128), f32),
            pltpu.VMEM((n, 128, own), f32),
            pltpu.VMEM((own, hv, hk), bf16),
            pltpu.VMEM((total, 2, hv, hk), bf16),
            pltpu.VMEM((total, hv, hk), bf16),
            pltpu.VMEM((total, 2, hv, hk), bf16),
            pltpu.VMEM((total, hv, hk), bf16),
            pltpu.VMEM((total, hv, hk), bf16),
            pltpu.VMEM((2, groups, seqs, hk), f32),
            pltpu.VMEM((groups, seqs, hk), f32),
            dma((9,)),
            dma((peers,)),
            dma((units, peers)),
            dma((3, peers)),
            dma((units, peers)),
            dma((1 + peers,)),
            dma((units,)),
            dma(()),
            dma((n - 1,)),
            dma((own,)),
            dma(()),
            dma((total,)),
            dma(()),
            dma((groups,)),
            dma(()),
            dma((total,)),
            dma(()),
            dma((total,)),
            pltpu.SemaphoreType.REGULAR,
            pltpu.SemaphoreType.REGULAR,
        ],
        compiler_params=pltpu.CompilerParams(
            collective_id=0,
            has_side_effects=True,
            vmem_limit_bytes=67043328 - rows * width * 4 - 2**18,
        ),
        cost_estimate=pl.CostEstimate(
            flops=6 * 10**9, bytes_accessed=2 * 10**7, transcendentals=10**6
        ),
    )(
        tokens,
        pre_gain[None, :],
        w_forget,
        w_value,
        w_query,
        w_gate,
        w_out,
        extra_decay,
        lower_bound[None, :],
        initial_state,
        norm_gain[None, :],
    )
    return (out * post_gain).astype(bf16).reshape(seqs, length, width)


def solution(mesh):
    in_specs = (
        P("dp", "sp", None),
        P(),
        P("dp", None),
        P("dp", None),
        P("dp", None),
        P("dp", None),
        P(),
        P(("dp", "sp"), None),
        P(("dp", "sp"), None, None),
        P(),
        P("dp", None),
        P(),
    )
    out_specs = P("dp", "sp", None)
    return jax.shard_map(
        functools.partial(body, mesh.shape["sp"], mesh.shape["dp"]),
        mesh=mesh,
        in_specs=in_specs,
        out_specs=out_specs,
        check_vma=False,
    )
```

```python
import functools

import jax
import jax.numpy as jnp
from jax import lax
from jax.experimental import pallas as pl
from jax.experimental.pallas import tpu as pltpu
from jax.sharding import PartitionSpec as P

EPS = 1e-06
MESH = pl.DeviceIdType.MESH
NT = (((1,), (1,)), ((), ()))
TN = (((0,), (0,)), ((), ()))


def rms_scale(matrix, gain):
    widened = matrix.astype(jnp.float32)
    return widened * lax.rsqrt(jnp.mean(widened * widened, axis=-1, keepdims=True) + EPS) * gain


def layer_kernel(
    n,
    ways,
    heads,
    axes,
    tokens_hbm,
    pre_hbm,
    wf_hbm,
    wv_hbm,
    wq_hbm,
    wg_hbm,
    wo_hbm,
    extra_hbm,
    bound_hbm,
    init_hbm,
    gain_hbm,
    out_ref,
    *scratch,
):
    units = len(axes)
    groups = heads // 2
    wholes = scratch[:units]
    (
        tokens_ref,
        pre_ref,
        raw_ref,
        bound_ref,
        start_ref,
        gain_ref,
        normed,
        f_ref,
        v_ref,
        q_ref,
        g_ref,
        keys_ref,
        rel_ref,
        gap_ref,
        emid_ref,
        eend_ref,
        within_ref,
        gated_ref,
        esend,
        erecv,
        extra_ref,
        isend,
        st,
        fin,
        bb,
        bs,
        ob,
        dbuf,
        dsend,
        local_sem,
        y_send,
        y_recv,
        r_send,
        r_recv,
        s_send,
        s_recv,
        e_send,
        e_recv,
        i_send,
        b_send,
        b_recv,
        d_send,
        d_recv,
        c_send,
        c_recv,
        t_send,
        t_recv,
        up_sem,
        down_sem,
    ) = scratch[units:]
    me = lax.axis_index("sp")
    rank = lax.axis_index("dp")
    seqs, length, width = tokens_ref.shape
    own, hk, hv = start_ref.shape
    half = 2 * hk
    total = groups * seqs
    levels = n // 2
    side = lax.rem(me, 2)
    level = me // 2
    parity = lax.rem(level, 2)
    beside = me + 1 - 2 * side
    above = lax.rem(me + 2, n)
    below = lax.rem(me + n - 2, n)
    sibling = rank + 1 - 2 * lax.rem(rank, 2)
    peers = ways // 2 - 1
    not_top = level < levels - 1
    not_base = level > 0
    second_top = level == levels - 2
    unit_f = 4
    unit_q = unit_f + 2 * (groups - 1)
    unit_g = unit_q + groups
    unit_o = unit_g + groups

    def group_cols(base, g):
        return base.at[:, g * half : (g + 1) * half]

    def source(u):
        if u < 4:
            base = wf_hbm if u % 2 == 0 else wv_hbm
            head = side if u >= 2 else 1 - side
            return base.at[:, pl.ds(pl.multiple_of(head * hk, hk), hk)]
        if u < unit_q:
            return group_cols(wf_hbm if u % 2 == 0 else wv_hbm, (u - unit_f) // 2 + 1)
        if u < unit_g:
            return group_cols(wq_hbm, u - unit_q)
        if u < unit_o:
            return group_cols(wg_hbm, u - unit_g)
        part = width // 2
        return wo_hbm.at[:, (u - unit_o) * part : (u - unit_o + 1) * part]

    def full(u, shard):
        rows = wholes[u].shape[0] // ways
        return wholes[u].at[pl.ds(pl.multiple_of(shard * rows, rows), rows)]

    def part(u, shard, which):
        rows = wholes[u].shape[0] // ways
        start = shard * rows + which * (rows // 2)
        return wholes[u].at[pl.ds(pl.multiple_of(start, rows // 2), rows // 2)]

    def local_copy(u):
        return pltpu.make_async_copy(source(u), full(u, rank), local_sem.at[min(u, 2)])

    small = [
        pltpu.make_async_copy(src, dst, local_sem.at[3 + j])
        for j, (src, dst) in enumerate(
            (
                (tokens_hbm, tokens_ref),
                (pre_hbm, pre_ref),
                (extra_hbm, raw_ref),
                (init_hbm, start_ref),
                (bound_hbm, bound_ref),
                (gain_hbm, gain_ref),
            )
        )
    ]
    for u in (0, 1):
        local_copy(u).start()
    small[0].start()
    small[1].start()
    for u in range(2, units):
        local_copy(u).start()
    for copy in small[2:]:
        copy.start()

    barrier = pltpu.get_barrier_semaphore()

    def greet(device):
        pl.semaphore_signal(barrier, inc=1, device_id=device, device_id_type=MESH)

    greet({"sp": beside})
    for offset in range(1, ways):
        greet({"dp": lax.rem(rank + offset, ways)})

    @pl.when(not_top)
    def _():
        greet({"sp": above})

    @pl.when(not_base)
    def _():
        greet({"sp": below})

    pl.semaphore_wait(
        barrier, ways + not_top.astype(jnp.int32) + not_base.astype(jnp.int32)
    )

    def remote(src, dst, send, recv, device):
        return pltpu.make_async_remote_copy(
            src_ref=src,
            dst_ref=dst,
            send_sem=send,
            recv_sem=recv,
            device_id=device,
            device_id_type=MESH,
        )

    def settle(sem, rows, ref=None):
        ref = out_ref if ref is None else ref
        if rows:
            view = ref.at[0:rows]
            pltpu.make_async_copy(view, view, sem).wait()

    def bulk(us, halves=False):
        line = width * 4
        size = sum(wholes[u].shape[0] // ways * wholes[u].shape[1] * 2 for u in us)
        return size // (2 if halves else 1) // line

    z_units = [u for u in range(units) if axes[u] == "z"]

    def first_part(u, shard):
        return part(u, shard, parity) if axes[u] == "z" else full(u, shard)

    def y_copy(u, k):
        ref = first_part(u, rank)
        target = lax.rem(rank + 2 * (k + 1), ways)
        return remote(ref, ref, y_send.at[k], y_recv.at[u, k], {"dp": target})

    def y_rest(u, k):
        ref = part(u, rank, 1 - parity)
        target = lax.rem(rank + 2 * (k + 1), ways)
        return remote(ref, ref, r_send.at[2, k], r_recv.at[u, k], {"dp": target})

    def origin(k):
        return lax.rem(rank + ways - 2 * (k + 1), ways)

    def m_copy(u, k):
        src, dst = full(u, origin(k)), full(u + 2, origin(k))
        return remote(src, dst, r_send.at[0, k], r_recv.at[u + 2, k], {"sp": beside})

    def z_copy(u, k, upward):
        ref = part(u, origin(k), parity)
        device = {"sp": above if upward else below}
        return remote(ref, ref, r_send.at[1 + upward, k], r_recv.at[u, k], device)

    def relay(u, k):
        if axes[u] == "y":
            m_copy(u, k).start()
        if axes[u] == "z":

            @pl.when(not_base)
            def _():
                z_copy(u, k, 0).start()

            if u < unit_g:

                @pl.when(second_top)
                def _():
                    z_copy(u, k, 1).start()

    def s_own(u):
        ref = full(u, rank)
        return remote(ref, ref, s_send.at[0], s_recv.at[u], {"dp": sibling})

    def s_copy(u, k, second):
        ref = part(u, origin(k), 1 - parity) if second else first_part(u, origin(k))
        return remote(ref, ref, s_send.at[1 + k], s_recv.at[u], {"dp": sibling})

    def pass_y(u):
        for k in range(peers):
            y_copy(u, k).wait_recv()
            relay(u, k)
            s_copy(u, k, 0).start()

    def pass_r(u):
        for k in range(peers):
            if axes[u] == "m":
                m_copy(u - 2, k).wait_recv()
                s_copy(u, k, 0).start()
            else:
                z_copy(u, k, 0).wait_recv()
                s_copy(u, k, 1).start()

    def arrived(u):
        settle(s_recv.at[u], wholes[u].shape[0] // 2, wholes[u])

    def e_copy(offset):
        target = lax.rem(me + offset, n)
        return remote(
            esend.at[target],
            erecv.at[me],
            e_send,
            e_recv.at[offset - 1],
            {"sp": target},
        )

    near = jnp.where(side == 0, 1, n - 1)

    def place(j):
        it = me * own + j
        h = lax.rem(it, heads)
        return lax.rem(h, 2), (h // 2) * seqs + it // heads

    def i_copy(j):
        target, k = place(j)
        return remote(isend.at[j], st.at[k, 0], i_send.at[j], c_recv.at[k], {"sp": target})

    def b_copy(k):
        return remote(bs.at[k], bb.at[k, side], b_send, b_recv.at[k], {"sp": beside})

    def d_copy(g):
        return remote(dsend.at[g], dbuf.at[side, g], d_send, d_recv.at[g], {"sp": beside})

    def c_copy(k):
        return remote(ob.at[k], st.at[k, 0], c_send, c_recv.at[k], {"sp": above})

    def t_copy(k):
        return remote(st.at[k, 1 - side], fin.at[k], t_send, t_recv.at[k], {"sp": beside})

    for u in range(units):
        if u < 2:
            local_copy(u).wait()
        if u == 2:
            settle(local_sem.at[2], bulk(range(2, units)))
        if axes[u] != "m":
            for k in range(peers):
                y_copy(u, k).start()
        s_own(u).start()

    @pl.when(jnp.logical_not(not_top))
    def _():
        for u in range(unit_g, units):
            for k in range(peers):
                y_rest(u, k).start()

    def tell(sem, device):
        pl.semaphore_signal(sem, inc=1, device_id={"sp": device}, device_id_type=MESH)

    @pl.when(jnp.logical_not(not_base))
    def _():
        tell(up_sem, above)

    @pl.when(jnp.logical_not(not_top))
    def _():
        tell(down_sem, below)

    for copy in small:
        copy.wait()

    def norm_rows(s, carry):
        rows = pl.ds(pl.multiple_of(s * length, length), length)
        normed[rows, :] = rms_scale(tokens_ref[s], pre_ref[...]).astype(jnp.bfloat16)
        return carry

    def send_extras(upward):
        for offset in range(1, n):
            there = lax.rem(me + offset, n) // 2
            far = there > level if upward else there < level

            @pl.when(far)
            def _():
                e_copy(offset).start()

    def send_states():
        for j in range(own):
            target, k = place(j)

            @pl.when(me != target)
            def _():
                i_copy(j).start()

            @pl.when(me == target)
            def _():
                st[k, 0] = isend[j]

    pad = esend.shape[2]
    for p in range(n):
        piece = raw_ref[:, p * length : (p + 1) * length]
        esend[p] = jnp.concatenate(
            [piece, jnp.zeros((own, pad - length), jnp.float32)], axis=1
        )
    for j in range(own):
        isend[j] = start_ref[j].T.astype(jnp.bfloat16)
    e_copy(near).start()

    @pl.when(not_base)
    def _():
        pl.semaphore_wait(up_sem, 1)

        @pl.when(not_top)
        def _():
            tell(up_sem, above)

        send_extras(False)

    send_states()
    for h in range(heads):
        gap_ref[h] = 1.0 - bound_ref[:, h * hk : (h + 1) * hk]
    erecv[me] = esend[me]
    lax.fori_loop(0, seqs, norm_rows, 0)

    @pl.when(jnp.logical_and(not_base, not_top))
    def _():
        pl.semaphore_wait(down_sem, 1)
        tell(down_sem, below)
        send_extras(True)

    pass_y(0)

    @pl.when(jnp.logical_not(not_base))
    def _():
        pl.semaphore_wait(down_sem, 1)
        send_extras(True)

    row = lax.broadcasted_iota(jnp.int32, (length, length), 0)
    col = lax.broadcasted_iota(jnp.int32, (length, length), 1)
    causal = row >= col
    ones = causal.astype(jnp.bfloat16)
    ones = jnp.concatenate([ones, ones], axis=1)
    middle = length // 2

    def seq_rows(s):
        return pl.ds(pl.multiple_of(s * length, length), length)

    def head_of(g, role):
        return 2 * g + (side if role == 0 else 1 - side)

    def head_lanes(g, role):
        return pl.ds(pl.multiple_of(head_of(g, role) * hk, hk), hk)

    def project(u, dest, lanes):
        dest[:, lanes] = jnp.dot(
            normed[...], wholes[u][...], preferred_element_type=jnp.float32
        ).astype(jnp.bfloat16)

    def group_lanes(g):
        return slice(g * half, (g + 1) * half)

    def extras(s):
        for j in range(heads // own):
            p = s * (heads // own) + j
            offset = lax.rem(me - p + n, n)

            @pl.when(offset > 0)
            def _():
                e_copy(offset).wait_recv()

            extra_ref[p] = erecv[p].T

    def decays(g, role, s):
        rows = seq_rows(s)
        lanes = head_lanes(g, role)
        head = head_of(g, role)
        keys = gap_ref[head] * jax.nn.sigmoid(-f_ref[rows, lanes].astype(jnp.float32))
        columns = [
            extra_ref[s * (heads // own) + h // own][:length, h % own : h % own + 1]
            for h in (2 * g, 2 * g + 1)
        ]
        spread = jnp.where(side == role, columns[0], columns[1])
        decay = jnp.log(1.0 - keys) + spread
        high = decay.astype(jnp.bfloat16)
        low = (decay - high.astype(jnp.float32)).astype(jnp.bfloat16)
        cum = jnp.dot(
            ones, jnp.concatenate([high, low], axis=0), preferred_element_type=jnp.float32
        )
        mid = cum[middle : middle + 1, :]
        end = cum[length - 1 : length, :]
        rel = cum - mid
        keys_ref[rows, lanes] = (keys * jnp.exp(-rel)).astype(jnp.bfloat16)
        rel_ref[rows, lanes] = rel
        emid_ref[head, pl.ds(s, 1)] = jnp.exp(mid)
        eend_ref[head, pl.ds(s, 1)] = jnp.exp(end - mid)
        if role == 0:
            dbuf[side, g, pl.ds(s, 1)] = jnp.exp(end)
        else:
            dsend[g, pl.ds(s, 1)] = jnp.exp(end)

    def added(g, role, s):
        rows = seq_rows(s)
        lanes = head_lanes(g, role)
        state = lax.dot_general(
            v_ref[rows, lanes], keys_ref[rows, lanes], TN, preferred_element_type=jnp.float32
        )
        return (state * eend_ref[head_of(g, role), pl.ds(s, 1)]).astype(jnp.bfloat16)

    def local_sent(g, s):
        k = g * seqs + s
        bs[k] = added(g, 1, s)
        b_copy(k).start()

    def local_kept(g, s):
        bb[g * seqs + s, side] = added(g, 0, s)

    def chain(k, carry):
        g = k // seqs
        s = lax.rem(k, seqs)
        holder = (s * heads + 2 * g + side) // own
        b_copy(k).wait_recv()

        @pl.when(jnp.logical_or(not_base, holder != me))
        def _():
            c_copy(k).wait_recv()

        first = dbuf[0, g, pl.ds(s, 1)]
        between = st[k, 0].astype(jnp.float32) * first + bb[k, 0].astype(jnp.float32)
        st[k, 1] = between.astype(jnp.bfloat16)
        t_copy(k).start()

        @pl.when(not_top)
        def _():
            second = dbuf[1, g, pl.ds(s, 1)]
            ob[k] = (between * second + bb[k, 1].astype(jnp.float32)).astype(jnp.bfloat16)
            c_copy(k).start()

        return carry

    def reached(g, time):
        begin = 182 + 81 * g + jnp.where(not_base, 10 + 22 * level, 0)
        return g * seqs + jnp.clip(time - begin + 7, 0, 7 * seqs) // 7

    def advance(before, now):
        for g in range(groups):
            lax.fori_loop(reached(g, before), reached(g, now), chain, 0)

    def intra(s):
        rows = seq_rows(s)
        for h in range(heads):
            lanes = slice(h * hk, (h + 1) * hk)
            q_pre = q_ref[rows, lanes].astype(jnp.float32)
            q_mid = q_pre * jax.nn.sigmoid(q_pre) * jnp.exp(rel_ref[rows, lanes])
            q_ref[rows, lanes] = (q_mid * emid_ref[h, pl.ds(s, 1)]).astype(jnp.bfloat16)
            scores = lax.dot_general(
                q_mid.astype(jnp.bfloat16),
                keys_ref[rows, lanes],
                NT,
                preferred_element_type=jnp.float32,
            )
            scores = jnp.where(causal, scores, 0.0).astype(jnp.bfloat16)
            within_ref[rows, lanes] = jnp.dot(
                scores, v_ref[rows, lanes], preferred_element_type=jnp.float32
            )

    def finish(t, carry):
        for b in range(2):
            s = 2 * t + b
            rows = seq_rows(s)
            for g in range(groups):
                k = g * seqs + s
                for role in range(2):
                    lanes = head_lanes(g, role)
                    state = st[k, side] if role == 0 else fin[k]
                    outs = within_ref[rows, lanes] + lax.dot_general(
                        q_ref[rows, lanes], state, NT, preferred_element_type=jnp.float32
                    )
                    scaled = rms_scale(outs, gain_ref[...]).astype(jnp.bfloat16)
                    g_pre = g_ref[rows, lanes].astype(jnp.float32)
                    gated_ref[b * length : (b + 1) * length, lanes] = (
                        scaled.astype(jnp.float32) * (g_pre * jax.nn.sigmoid(g_pre))
                    ).astype(jnp.bfloat16)
        tile = 512
        squares = jnp.zeros((2 * length, 1), jnp.float32)
        rows = pl.ds(pl.multiple_of(t * 2 * length, 2 * length), 2 * length)
        tiles = [
            (unit_o + p, slice(j * tile, (j + 1) * tile), p * (width // 2) + j * tile)
            for p in range(2)
            for j in range(width // 2 // tile)
        ]
        for u, lanes, at in tiles:
            mixed = jnp.dot(
                gated_ref[...], wholes[u][:, lanes], preferred_element_type=jnp.float32
            )
            squares = squares + jnp.sum(mixed * mixed, axis=-1, keepdims=True)
            out_ref[rows, at : at + tile] = mixed
        scale = lax.rsqrt(squares * (1.0 / width) + EPS)
        for u, lanes, at in tiles:
            out_ref[rows, at : at + tile] = out_ref[rows, at : at + tile] * scale
        return carry

    def loop(step, hooks=(), count=seqs):
        def run(s, carry):
            step(s)
            for at, act in hooks:

                @pl.when(s == at)
                def _():
                    act()

            return carry

        lax.fori_loop(0, count, run, 0)

    def paired(step):
        def run(t):
            step(2 * t)
            step(2 * t + 1)

        return run

    twos = seqs // 2
    arrived(0)
    project(0, f_ref, head_lanes(0, 1))
    pass_y(1)

    def first_decays(t):
        for s in (2 * t, 2 * t + 1):
            extras(s)
        for s in (2 * t, 2 * t + 1):
            decays(0, 1, s)

    loop(first_decays, count=twos)
    d_copy(0).start()
    arrived(1)
    project(1, v_ref, head_lanes(0, 1))
    pass_y(4)
    loop(paired(lambda s: local_sent(0, s)), count=twos)
    pass_r(2)
    arrived(2)
    project(2, f_ref, head_lanes(0, 0))
    loop(paired(lambda s: decays(0, 0, s)), ((twos - 1, lambda: pass_r(3)),), count=twos)
    pass_y(5)
    arrived(3)
    project(3, v_ref, head_lanes(0, 0))
    d_copy(0).wait_recv()
    loop(paired(lambda s: local_kept(0, s)), count=twos)
    advance(0, 197)
    pass_r(4)
    pass_y(6)
    arrived(4)
    project(4, f_ref, group_lanes(1))
    advance(197, 205)

    def later_other(t):
        decays(1, 1, 2 * t)
        decays(1, 1, 2 * t + 1)
        advance(205 + 3 * t, 208 + 3 * t)

    def later_mine(t):
        decays(1, 0, 2 * t)
        decays(1, 0, 2 * t + 1)
        advance(239 + 3 * t, 242 + 3 * t)

    def later_sent(t):
        local_sent(1, 2 * t)
        local_sent(1, 2 * t + 1)
        advance(227 + 3 * t, 230 + 3 * t)

    def later_kept(t):
        local_kept(1, 2 * t)
        local_kept(1, 2 * t + 1)
        advance(251 + 3 * t, 254 + 3 * t)

    loop(later_other, count=twos)
    d_copy(1).start()
    pass_r(5)
    pass_y(7)
    advance(205 + 3 * twos, 224)
    arrived(5)
    project(5, v_ref, group_lanes(1))
    advance(224, 227)
    pass_y(8)
    loop(later_sent, count=twos)
    loop(later_mine, count=twos)
    pass_y(9)
    pass_r(6)
    d_copy(1).wait_recv()
    loop(later_kept, count=twos)
    pass_y(10)
    time = 251 + 3 * twos
    advance(time, time + 1)
    pass_r(7)
    arrived(6)
    project(6, q_ref, group_lanes(0))
    advance(time + 1, 275)
    arrived(7)
    project(7, q_ref, group_lanes(1))
    advance(275, 293)
    pass_y(11)

    def intra_slot(s):
        intra(s)
        advance(293 + 6 * s, 299 + 6 * s)

    loop(
        intra_slot,
        (
            (seqs // 2, lambda: pass_r(8)),
            (seqs - 1, lambda: pass_r(9)),
        ),
    )
    time = 293 + 6 * seqs
    arrived(8)
    project(8, g_ref, group_lanes(0))
    advance(time, 356)
    arrived(9)
    project(9, g_ref, group_lanes(1))
    advance(356, 368)
    lax.fori_loop(reached(0, 368), seqs, chain, 0)
    done = jnp.where(not_top, total, reached(1, 368))
    lax.fori_loop(reached(1, 368), done, chain, 0)
    pass_r(10)
    pass_r(11)

    settle(e_send, n - 1, esend)
    for j in range(own):
        holder_target, _ = place(j)

        @pl.when(me != holder_target)
        def _():
            i_copy(j).wait_send()

    settle(d_send, groups, dsend)
    settle(b_send, total, bs)
    settle(s_send.at[0], bulk(range(units)))
    for k in range(peers):
        settle(y_send.at[k], bulk((0, 1)) + bulk(z_units, True))
        settle(r_send.at[0, k], bulk((0, 1)))
        settle(s_send.at[1 + k], bulk(range(units)))

        @pl.when(not_base)
        def _():
            settle(r_send.at[1, k], bulk(z_units, True))

        @pl.when(second_top)
        def _():
            settle(r_send.at[2, k], bulk(range(unit_f, unit_g), True))

        @pl.when(jnp.logical_not(not_top))
        def _():
            settle(r_send.at[2, k], bulk(range(unit_g, units), True))

    arrived(10)
    arrived(11)

    def ending(t, carry):
        def goal(t):
            return jnp.maximum(seqs + jnp.minimum(2 * t + 4, seqs), done)

        lax.fori_loop(jnp.where(t == 0, done, goal(t - 1)), goal(t), chain, 0)
        for g in range(groups):
            for b in range(2):
                t_copy(g * seqs + 2 * t + b).wait_recv()
        return finish(t, carry)

    lax.fori_loop(0, seqs // 2, ending, 0)

    settle(t_send, total, fin)

    @pl.when(not_top)
    def _():
        settle(c_send, total, ob)


def body(
    n,
    ways,
    tokens,
    pre_gain,
    w_query,
    w_forget,
    w_value,
    w_gate,
    lower_bound,
    extra_decay,
    initial_state,
    norm_gain,
    w_out,
    post_gain,
):
    seqs, length, width = tokens.shape
    own, hk, hv = initial_state.shape
    items = own * n
    heads = items // seqs
    groups = heads // 2
    half = 2 * hk
    cols = heads * hk
    rows = seqs * length
    total = groups * seqs
    peers = max(ways // 2 - 1, 1)
    axes = ("y", "y", "m", "m") + ("z",) * (2 * (groups - 1) + 2 * groups + 2)
    units = len(axes)
    dma = pltpu.SemaphoreType.DMA
    bf16, f32 = jnp.bfloat16, jnp.float32
    shapes = [(width, hk)] * 4 + [(width, half)] * (4 * groups - 2) + [(cols, width // 2)] * 2
    out = pl.pallas_call(
        functools.partial(layer_kernel, n, ways, heads, axes),
        out_shape=pltpu.VMEM((rows, width), f32),
        in_specs=[pl.BlockSpec(memory_space=pltpu.HBM)] * 11,
        out_specs=pl.BlockSpec(memory_space=pltpu.VMEM),
        scratch_shapes=[pltpu.VMEM(shape, bf16) for shape in shapes]
        + [
            pltpu.VMEM(tokens.shape, bf16),
            pltpu.VMEM((1, width), f32),
            pltpu.VMEM(extra_decay.shape, f32),
            pltpu.VMEM((1, cols), f32),
            pltpu.VMEM(initial_state.shape, f32),
            pltpu.VMEM((1, hv), f32),
            pltpu.VMEM((rows, width), bf16),
            pltpu.VMEM((rows, cols), bf16),
            pltpu.VMEM((rows, cols), bf16),
            pltpu.VMEM((rows, cols), bf16),
            pltpu.VMEM((rows, cols), bf16),
            pltpu.VMEM((rows, cols), bf16),
            pltpu.VMEM((rows, cols), f32),
            pltpu.VMEM((heads, 1, hk), f32),
            pltpu.VMEM((heads, seqs, hk), f32),
            pltpu.VMEM((heads, seqs, hk), f32),
            pltpu.VMEM((rows, cols), f32),
            pltpu.VMEM((2 * length, cols), bf16),
            pltpu.VMEM((n, own, 128), f32),
            pltpu.VMEM((n, own, 128), f32),
            pltpu.VMEM((n, 128, own), f32),
            pltpu.VMEM((own, hv, hk), bf16),
            pltpu.VMEM((total, 2, hv, hk), bf16),
            pltpu.VMEM((total, hv, hk), bf16),
            pltpu.VMEM((total, 2, hv, hk), bf16),
            pltpu.VMEM((total, hv, hk), bf16),
            pltpu.VMEM((total, hv, hk), bf16),
            pltpu.VMEM((2, groups, seqs, hk), f32),
            pltpu.VMEM((groups, seqs, hk), f32),
            dma((9,)),
            dma((peers,)),
            dma((units, peers)),
            dma((3, peers)),
            dma((units, peers)),
            dma((1 + peers,)),
            dma((units,)),
            dma(()),
            dma((n - 1,)),
            dma((own,)),
            dma(()),
            dma((total,)),
            dma(()),
            dma((groups,)),
            dma(()),
            dma((total,)),
            dma(()),
            dma((total,)),
            pltpu.SemaphoreType.REGULAR,
            pltpu.SemaphoreType.REGULAR,
        ],
        compiler_params=pltpu.CompilerParams(
            collective_id=0,
            has_side_effects=True,
            vmem_limit_bytes=67043328 - rows * width * 4 - 2**18,
        ),
        cost_estimate=pl.CostEstimate(
            flops=6 * 10**9, bytes_accessed=2 * 10**7, transcendentals=10**6
        ),
    )(
        tokens,
        pre_gain[None, :],
        w_forget,
        w_value,
        w_query,
        w_gate,
        w_out,
        extra_decay,
        lower_bound[None, :],
        initial_state,
        norm_gain[None, :],
    )
    return (out * post_gain).astype(bf16).reshape(seqs, length, width)


def solution(mesh):
    in_specs = (
        P("dp", "sp", None),
        P(),
        P("dp", None),
        P("dp", None),
        P("dp", None),
        P("dp", None),
        P(),
        P(("dp", "sp"), None),
        P(("dp", "sp"), None, None),
        P(),
        P("dp", None),
        P(),
    )
    out_specs = P("dp", "sp", None)
    return jax.shard_map(
        functools.partial(body, mesh.shape["sp"], mesh.shape["dp"]),
        mesh=mesh,
        in_specs=in_specs,
        out_specs=out_specs,
        check_vma=False,
    )
```

```python
import functools

import jax
import jax.numpy as jnp
from jax import lax
from jax.experimental import pallas as pl
from jax.experimental.pallas import tpu as pltpu
from jax.sharding import PartitionSpec as P

EPS = 1e-06
MESH = pl.DeviceIdType.MESH
NT = (((1,), (1,)), ((), ()))
TN = (((0,), (0,)), ((), ()))


def rms_scale(matrix, gain):
    widened = matrix.astype(jnp.float32)
    return widened * lax.rsqrt(jnp.mean(widened * widened, axis=-1, keepdims=True) + EPS) * gain


def layer_kernel(
    n,
    ways,
    heads,
    axes,
    tokens_hbm,
    pre_hbm,
    wf_hbm,
    wv_hbm,
    wq_hbm,
    wg_hbm,
    wo_hbm,
    extra_hbm,
    bound_hbm,
    init_hbm,
    gain_hbm,
    post_hbm,
    out_ref,
    *scratch,
):
    units = len(axes)
    groups = heads // 2
    wholes = scratch[:units]
    (
        tokens_ref,
        pre_ref,
        raw_ref,
        bound_ref,
        start_ref,
        gain_ref,
        post_ref,
        mixed_ref,
        normed,
        f_ref,
        v_ref,
        q_ref,
        g_ref,
        keys_ref,
        rel_ref,
        gap_ref,
        emid_ref,
        eend_ref,
        within_ref,
        gated_ref,
        esend,
        erecv,
        extra_ref,
        isend,
        st,
        fin,
        bb,
        bs,
        ob,
        dbuf,
        dsend,
        local_sem,
        y_send,
        y_recv,
        r_send,
        r_recv,
        s_send,
        s_recv,
        e_send,
        e_recv,
        i_send,
        b_send,
        b_recv,
        d_send,
        d_recv,
        c_send,
        c_recv,
        t_send,
        t_recv,
        up_sem,
        down_sem,
    ) = scratch[units:]
    me = lax.axis_index("sp")
    rank = lax.axis_index("dp")
    seqs, length, width = tokens_ref.shape
    own, hk, hv = start_ref.shape
    half = 2 * hk
    total = groups * seqs
    levels = n // 2
    side = lax.rem(me, 2)
    level = me // 2
    parity = lax.rem(level, 2)
    beside = me + 1 - 2 * side
    above = lax.rem(me + 2, n)
    below = lax.rem(me + n - 2, n)
    sibling = rank + 1 - 2 * lax.rem(rank, 2)
    peers = ways // 2 - 1
    not_top = level < levels - 1
    not_base = level > 0
    second_top = level == levels - 2
    unit_f = 4
    unit_q = unit_f + 2 * (groups - 1)
    unit_g = unit_q + groups
    unit_o = unit_g + groups

    def group_cols(base, g):
        return base.at[:, g * half : (g + 1) * half]

    def source(u):
        if u < 4:
            base = wf_hbm if u % 2 == 0 else wv_hbm
            head = side if u >= 2 else 1 - side
            return base.at[:, pl.ds(pl.multiple_of(head * hk, hk), hk)]
        if u < unit_q:
            return group_cols(wf_hbm if u % 2 == 0 else wv_hbm, (u - unit_f) // 2 + 1)
        if u < unit_g:
            return group_cols(wq_hbm, u - unit_q)
        if u < unit_o:
            return group_cols(wg_hbm, u - unit_g)
        part = width // 2
        return wo_hbm.at[:, (u - unit_o) * part : (u - unit_o + 1) * part]

    def full(u, shard):
        rows = wholes[u].shape[0] // ways
        return wholes[u].at[pl.ds(pl.multiple_of(shard * rows, rows), rows)]

    def part(u, shard, which):
        rows = wholes[u].shape[0] // ways
        start = shard * rows + which * (rows // 2)
        return wholes[u].at[pl.ds(pl.multiple_of(start, rows // 2), rows // 2)]

    def local_copy(u):
        return pltpu.make_async_copy(source(u), full(u, rank), local_sem.at[3 if u >= unit_g else min(u, 2)])

    small = [
        pltpu.make_async_copy(src, dst, local_sem.at[4 + j])
        for j, (src, dst) in enumerate(
            (
                (tokens_hbm, tokens_ref),
                (pre_hbm, pre_ref),
                (extra_hbm, raw_ref),
                (init_hbm, start_ref),
                (bound_hbm, bound_ref),
                (gain_hbm, gain_ref),
                (post_hbm, post_ref),
            )
        )
    ]
    for u in (0, 1):
        local_copy(u).start()
    small[0].start()
    small[1].start()
    for u in range(2, units):
        local_copy(u).start()
    for copy in small[2:]:
        copy.start()

    barrier = pltpu.get_barrier_semaphore()

    def greet(device):
        pl.semaphore_signal(barrier, inc=1, device_id=device, device_id_type=MESH)

    greet({"sp": beside})
    for offset in range(1, ways):
        greet({"dp": lax.rem(rank + offset, ways)})

    @pl.when(not_top)
    def _():
        greet({"sp": above})

    @pl.when(not_base)
    def _():
        greet({"sp": below})

    pl.semaphore_wait(
        barrier, ways + not_top.astype(jnp.int32) + not_base.astype(jnp.int32)
    )

    def remote(src, dst, send, recv, device):
        return pltpu.make_async_remote_copy(
            src_ref=src,
            dst_ref=dst,
            send_sem=send,
            recv_sem=recv,
            device_id=device,
            device_id_type=MESH,
        )

    def settle(sem, rows, ref=None):
        ref = out_ref if ref is None else ref
        if rows:
            view = ref.at[0:rows]
            pltpu.make_async_copy(view, view, sem).wait()

    def bulk(us, halves=False):
        line = width * 2
        size = sum(wholes[u].shape[0] // ways * wholes[u].shape[1] * 2 for u in us)
        return size // (2 if halves else 1) // line

    z_units = [u for u in range(units) if axes[u] == "z"]

    def first_part(u, shard):
        return part(u, shard, parity) if axes[u] == "z" else full(u, shard)

    def y_copy(u, k):
        ref = first_part(u, rank)
        target = lax.rem(rank + 2 * (k + 1), ways)
        return remote(ref, ref, y_send.at[k], y_recv.at[u, k], {"dp": target})

    def y_rest(u, k):
        ref = part(u, rank, 1 - parity)
        target = lax.rem(rank + 2 * (k + 1), ways)
        return remote(ref, ref, r_send.at[2, k], r_recv.at[u, k], {"dp": target})

    def origin(k):
        return lax.rem(rank + ways - 2 * (k + 1), ways)

    def m_copy(u, k):
        src, dst = full(u, origin(k)), full(u + 2, origin(k))
        return remote(src, dst, r_send.at[0, k], r_recv.at[u + 2, k], {"sp": beside})

    def z_copy(u, k, upward):
        ref = part(u, origin(k), parity)
        device = {"sp": above if upward else below}
        return remote(ref, ref, r_send.at[1 + upward, k], r_recv.at[u, k], device)

    def relay(u, k):
        if axes[u] == "y":
            m_copy(u, k).start()
        if axes[u] == "z":

            @pl.when(not_base)
            def _():
                z_copy(u, k, 0).start()

            if u < unit_g:

                @pl.when(second_top)
                def _():
                    z_copy(u, k, 1).start()

    def s_own(u):
        ref = full(u, rank)
        return remote(ref, ref, s_send.at[u // unit_g, 0], s_recv.at[u], {"dp": sibling})

    def s_copy(u, k, second):
        ref = part(u, origin(k), 1 - parity) if second else first_part(u, origin(k))
        return remote(ref, ref, s_send.at[u // unit_g, 1 + k], s_recv.at[u], {"dp": sibling})

    def pass_y(u):
        for k in range(peers):
            y_copy(u, k).wait_recv()
            relay(u, k)
            s_copy(u, k, 0).start()

    def pass_r(u):
        for k in range(peers):
            if axes[u] == "m":
                m_copy(u - 2, k).wait_recv()
                s_copy(u, k, 0).start()
            else:
                z_copy(u, k, 0).wait_recv()
                s_copy(u, k, 1).start()

    def arrived(u):
        settle(s_recv.at[u], wholes[u].shape[0] // 2, wholes[u])

    def e_copy(offset):
        target = lax.rem(me + offset, n)
        return remote(
            esend.at[target],
            erecv.at[me],
            e_send,
            e_recv.at[offset - 1],
            {"sp": target},
        )

    near = jnp.where(side == 0, 1, n - 1)

    def place(j):
        it = me * own + j
        h = lax.rem(it, heads)
        return lax.rem(h, 2), (h // 2) * seqs + it // heads

    def i_copy(j):
        target, k = place(j)
        return remote(isend.at[j], st.at[k, 0], i_send.at[j], c_recv.at[k], {"sp": target})

    def b_copy(k):
        return remote(bs.at[k], bb.at[k, side], b_send, b_recv.at[k], {"sp": beside})

    def d_copy(g):
        return remote(dsend.at[g], dbuf.at[side, g], d_send, d_recv.at[g], {"sp": beside})

    def c_copy(k):
        return remote(ob.at[k], st.at[k, 0], c_send, c_recv.at[k], {"sp": above})

    def t_copy(k):
        return remote(st.at[k, 1 - side], fin.at[k], t_send, t_recv.at[k], {"sp": beside})

    for u in range(units):
        if u < 2:
            local_copy(u).wait()
        if u == 2:
            settle(local_sem.at[2], bulk(range(2, unit_g)))
        if u == unit_g:
            settle(local_sem.at[3], bulk(range(unit_g, units)))
        if axes[u] != "m":
            for k in range(peers):
                y_copy(u, k).start()
        s_own(u).start()

    @pl.when(jnp.logical_not(not_top))
    def _():
        for u in range(unit_g, units):
            for k in range(peers):
                y_rest(u, k).start()

    def tell(sem, device):
        pl.semaphore_signal(sem, inc=1, device_id={"sp": device}, device_id_type=MESH)

    @pl.when(jnp.logical_not(not_base))
    def _():
        tell(up_sem, above)

    @pl.when(jnp.logical_not(not_top))
    def _():
        tell(down_sem, below)

    for copy in small:
        copy.wait()

    def norm_rows(s, carry):
        rows = pl.ds(pl.multiple_of(s * length, length), length)
        normed[rows, :] = rms_scale(tokens_ref[s], pre_ref[...]).astype(jnp.bfloat16)
        return carry

    def send_extras(upward):
        for offset in range(1, n):
            there = lax.rem(me + offset, n) // 2
            far = there > level if upward else there < level

            @pl.when(far)
            def _():
                e_copy(offset).start()

    def send_states():
        for j in range(own):
            target, k = place(j)

            @pl.when(me != target)
            def _():
                i_copy(j).start()

            @pl.when(me == target)
            def _():
                st[k, 0] = isend[j]

    pad = esend.shape[2]
    for p in range(n):
        piece = raw_ref[:, p * length : (p + 1) * length]
        esend[p] = jnp.concatenate(
            [piece, jnp.zeros((own, pad - length), jnp.float32)], axis=1
        )
    for j in range(own):
        isend[j] = start_ref[j].T.astype(jnp.bfloat16)
    e_copy(near).start()

    @pl.when(not_base)
    def _():
        pl.semaphore_wait(up_sem, 1)

        @pl.when(not_top)
        def _():
            tell(up_sem, above)

        send_extras(False)

    send_states()
    for h in range(heads):
        gap_ref[h] = 1.0 - bound_ref[:, h * hk : (h + 1) * hk]
    erecv[me] = esend[me]
    lax.fori_loop(0, seqs, norm_rows, 0)

    @pl.when(jnp.logical_and(not_base, not_top))
    def _():
        pl.semaphore_wait(down_sem, 1)
        tell(down_sem, below)
        send_extras(True)

    pass_y(0)

    @pl.when(jnp.logical_not(not_base))
    def _():
        pl.semaphore_wait(down_sem, 1)
        send_extras(True)

    row = lax.broadcasted_iota(jnp.int32, (length, length), 0)
    col = lax.broadcasted_iota(jnp.int32, (length, length), 1)
    causal = row >= col
    ones = causal.astype(jnp.bfloat16)
    ones = jnp.concatenate([ones, ones], axis=1)
    middle = length // 2

    def seq_rows(s):
        return pl.ds(pl.multiple_of(s * length, length), length)

    def head_of(g, role):
        return 2 * g + (side if role == 0 else 1 - side)

    def head_lanes(g, role):
        return pl.ds(pl.multiple_of(head_of(g, role) * hk, hk), hk)

    def project(u, dest, lanes):
        dest[:, lanes] = jnp.dot(
            normed[...], wholes[u][...], preferred_element_type=jnp.float32
        ).astype(jnp.bfloat16)

    def group_lanes(g):
        return slice(g * half, (g + 1) * half)

    def extras(s):
        for j in range(heads // own):
            p = s * (heads // own) + j
            offset = lax.rem(me - p + n, n)

            @pl.when(offset > 0)
            def _():
                e_copy(offset).wait_recv()

            extra_ref[p] = erecv[p].T

    def decays(g, role, s):
        rows = seq_rows(s)
        lanes = head_lanes(g, role)
        head = head_of(g, role)
        keys = gap_ref[head] * jax.nn.sigmoid(-f_ref[rows, lanes].astype(jnp.float32))
        columns = [
            extra_ref[s * (heads // own) + h // own][:length, h % own : h % own + 1]
            for h in (2 * g, 2 * g + 1)
        ]
        spread = jnp.where(side == role, columns[0], columns[1])
        decay = jnp.log(1.0 - keys) + spread
        high = decay.astype(jnp.bfloat16)
        low = (decay - high.astype(jnp.float32)).astype(jnp.bfloat16)
        cum = jnp.dot(
            ones, jnp.concatenate([high, low], axis=0), preferred_element_type=jnp.float32
        )
        mid = cum[middle : middle + 1, :]
        end = cum[length - 1 : length, :]
        rel = cum - mid
        keys_ref[rows, lanes] = (keys * jnp.exp(-rel)).astype(jnp.bfloat16)
        rel_ref[rows, lanes] = rel
        emid_ref[head, pl.ds(s, 1)] = jnp.exp(mid)
        eend_ref[head, pl.ds(s, 1)] = jnp.exp(end - mid)
        if role == 0:
            dbuf[side, g, pl.ds(s, 1)] = jnp.exp(end)
        else:
            dsend[g, pl.ds(s, 1)] = jnp.exp(end)

    def added(g, role, s):
        rows = seq_rows(s)
        lanes = head_lanes(g, role)
        state = lax.dot_general(
            v_ref[rows, lanes], keys_ref[rows, lanes], TN, preferred_element_type=jnp.float32
        )
        return (state * eend_ref[head_of(g, role), pl.ds(s, 1)]).astype(jnp.bfloat16)

    def local_sent(g, s):
        k = g * seqs + s
        bs[k] = added(g, 1, s)
        b_copy(k).start()

    def local_kept(g, s):
        bb[g * seqs + s, side] = added(g, 0, s)

    def chain(k, carry):
        g = k // seqs
        s = lax.rem(k, seqs)
        holder = (s * heads + 2 * g + side) // own
        b_copy(k).wait_recv()

        @pl.when(jnp.logical_or(not_base, holder != me))
        def _():
            c_copy(k).wait_recv()

        first = dbuf[0, g, pl.ds(s, 1)]
        between = st[k, 0].astype(jnp.float32) * first + bb[k, 0].astype(jnp.float32)
        st[k, 1] = between.astype(jnp.bfloat16)
        t_copy(k).start()

        @pl.when(not_top)
        def _():
            second = dbuf[1, g, pl.ds(s, 1)]
            ob[k] = (between * second + bb[k, 1].astype(jnp.float32)).astype(jnp.bfloat16)
            c_copy(k).start()

        return carry

    def reached(g, time):
        first, lag, hop = ((182, 10, 22), (258, 17, 20))[min(g, 1)]
        begin = first + jnp.where(not_base, lag + hop * level, 0)
        return g * seqs + jnp.clip(time - begin + 7, 0, 7 * seqs) // 7

    def advance(before, now):
        for g in range(groups):
            lax.fori_loop(reached(g, before), reached(g, now), chain, 0)

    def intra(s):
        rows = seq_rows(s)
        for h in range(heads):
            lanes = slice(h * hk, (h + 1) * hk)
            q_pre = q_ref[rows, lanes].astype(jnp.float32)
            q_mid = q_pre * jax.nn.sigmoid(q_pre) * jnp.exp(rel_ref[rows, lanes])
            q_ref[rows, lanes] = (q_mid * emid_ref[h, pl.ds(s, 1)]).astype(jnp.bfloat16)
            scores = lax.dot_general(
                q_mid.astype(jnp.bfloat16),
                keys_ref[rows, lanes],
                NT,
                preferred_element_type=jnp.float32,
            )
            scores = jnp.where(causal, scores, 0.0).astype(jnp.bfloat16)
            within_ref[rows, lanes] = jnp.dot(
                scores, v_ref[rows, lanes], preferred_element_type=jnp.float32
            )

    def finish(t, carry):
        for b in range(2):
            s = 2 * t + b
            rows = seq_rows(s)
            for g in range(groups):
                k = g * seqs + s
                for role in range(2):
                    lanes = head_lanes(g, role)
                    state = st[k, side] if role == 0 else fin[k]
                    outs = within_ref[rows, lanes] + lax.dot_general(
                        q_ref[rows, lanes], state, NT, preferred_element_type=jnp.float32
                    )
                    scaled = rms_scale(outs, gain_ref[...]).astype(jnp.bfloat16)
                    g_pre = g_ref[rows, lanes].astype(jnp.float32)
                    gated_ref[b * length : (b + 1) * length, lanes] = (
                        scaled.astype(jnp.float32) * (g_pre * jax.nn.sigmoid(g_pre))
                    ).astype(jnp.bfloat16)
        tile = 512
        squares = jnp.zeros((2 * length, 1), jnp.float32)
        rows = pl.ds(pl.multiple_of(t * 2 * length, 2 * length), 2 * length)
        tiles = [
            (unit_o + p, slice(j * tile, (j + 1) * tile), p * (width // 2) + j * tile)
            for p in range(2)
            for j in range(width // 2 // tile)
        ]
        for u, lanes, at in tiles:
            mixed = jnp.dot(
                gated_ref[...], wholes[u][:, lanes], preferred_element_type=jnp.float32
            )
            squares = squares + jnp.sum(mixed * mixed, axis=-1, keepdims=True)
            mixed_ref[:, at : at + tile] = mixed
        scale = lax.rsqrt(squares * (1.0 / width) + EPS)
        for u, lanes, at in tiles:
            out_ref[rows, at : at + tile] = (
                mixed_ref[:, at : at + tile] * scale * post_ref[:, at : at + tile]
            ).astype(jnp.bfloat16)
        return carry

    def loop(step, hooks=(), count=seqs):
        def run(s, carry):
            step(s)
            for at, act in hooks:

                @pl.when(s == at)
                def _():
                    act()

            return carry

        lax.fori_loop(0, count, run, 0)

    def paired(step):
        def run(t):
            step(2 * t)
            step(2 * t + 1)

        return run

    twos = seqs // 2
    arrived(0)
    project(0, f_ref, head_lanes(0, 1))
    pass_y(1)

    def first_decays(t):
        for s in (2 * t, 2 * t + 1):
            extras(s)
        for s in (2 * t, 2 * t + 1):
            decays(0, 1, s)

    loop(first_decays, count=twos)
    d_copy(0).start()
    arrived(1)
    project(1, v_ref, head_lanes(0, 1))
    pass_y(4)
    loop(paired(lambda s: local_sent(0, s)), count=twos)
    pass_r(2)
    arrived(2)
    project(2, f_ref, head_lanes(0, 0))
    loop(paired(lambda s: decays(0, 0, s)), ((1, lambda: pass_y(5)), (twos - 1, lambda: pass_r(3))), count=twos)
    arrived(3)
    project(3, v_ref, head_lanes(0, 0))
    d_copy(0).wait_recv()
    loop(paired(lambda s: local_kept(0, s)), count=twos)
    advance(0, 197)
    pass_r(4)
    pass_y(6)
    arrived(4)
    project(4, f_ref, group_lanes(1))
    advance(197, 205)

    def later_other(t):
        decays(1, 1, 2 * t)
        decays(1, 1, 2 * t + 1)
        advance(205 + 3 * t, 208 + 3 * t)

    def later_mine(t):
        decays(1, 0, 2 * t)
        decays(1, 0, 2 * t + 1)
        advance(239 + 3 * t, 242 + 3 * t)

    def later_sent(t):
        local_sent(1, 2 * t)
        local_sent(1, 2 * t + 1)
        advance(227 + 3 * t, 230 + 3 * t)

    def later_kept(t):
        local_kept(1, 2 * t)
        local_kept(1, 2 * t + 1)
        advance(251 + 3 * t, 254 + 3 * t)

    loop(later_other, count=twos)
    d_copy(1).start()
    pass_r(5)
    pass_y(7)
    advance(205 + 3 * twos, 224)
    arrived(5)
    project(5, v_ref, group_lanes(1))
    advance(224, 227)
    pass_y(8)
    loop(later_sent, count=twos)
    loop(later_mine, count=twos)
    pass_y(9)
    pass_r(6)
    d_copy(1).wait_recv()
    loop(later_kept, count=twos)
    pass_y(10)
    time = 251 + 3 * twos
    advance(time, time + 1)
    pass_r(7)
    arrived(6)
    project(6, q_ref, group_lanes(0))
    advance(time + 1, 275)
    arrived(7)
    project(7, q_ref, group_lanes(1))
    advance(275, 293)
    pass_y(11)

    def intra_slot(s):
        intra(s)
        advance(293 + 6 * s, 299 + 6 * s)

    loop(
        intra_slot,
        (
            (seqs // 2, lambda: pass_r(8)),
            (seqs - 1, lambda: pass_r(9)),
        ),
    )
    time = 293 + 6 * seqs
    arrived(8)
    project(8, g_ref, group_lanes(0))
    advance(time, time + 15)
    arrived(9)
    project(9, g_ref, group_lanes(1))
    advance(time + 15, time + 27)
    lax.fori_loop(reached(0, time + 27), seqs, chain, 0)
    lax.fori_loop(reached(1, time + 27), total, chain, 0)
    pass_r(10)
    pass_r(11)

    settle(e_send, n - 1, esend)
    for j in range(own):
        holder_target, _ = place(j)

        @pl.when(me != holder_target)
        def _():
            i_copy(j).wait_send()

    settle(d_send, groups, dsend)
    settle(b_send, total, bs)
    for later, us in enumerate((range(unit_g), range(unit_g, units))):
        settle(s_send.at[later, 0], bulk(us))
        for k in range(peers):
            settle(s_send.at[later, 1 + k], bulk(us))
    for k in range(peers):
        settle(y_send.at[k], bulk((0, 1)) + bulk(z_units, True))
        settle(r_send.at[0, k], bulk((0, 1)))

        @pl.when(not_base)
        def _():
            settle(r_send.at[1, k], bulk(z_units, True))

        @pl.when(second_top)
        def _():
            settle(r_send.at[2, k], bulk(range(unit_f, unit_g), True))

        @pl.when(jnp.logical_not(not_top))
        def _():
            settle(r_send.at[2, k], bulk(range(unit_g, units), True))

    arrived(10)
    arrived(11)

    def ending(t, carry):
        for g in range(groups):
            for b in range(2):
                t_copy(g * seqs + 2 * t + b).wait_recv()
        return finish(t, carry)

    lax.fori_loop(0, seqs // 2, ending, 0)

    settle(t_send, total, fin)

    @pl.when(not_top)
    def _():
        settle(c_send, total, ob)


def body(
    n,
    ways,
    tokens,
    pre_gain,
    w_query,
    w_forget,
    w_value,
    w_gate,
    lower_bound,
    extra_decay,
    initial_state,
    norm_gain,
    w_out,
    post_gain,
):
    seqs, length, width = tokens.shape
    own, hk, hv = initial_state.shape
    items = own * n
    heads = items // seqs
    groups = heads // 2
    half = 2 * hk
    cols = heads * hk
    rows = seqs * length
    total = groups * seqs
    peers = max(ways // 2 - 1, 1)
    axes = ("y", "y", "m", "m") + ("z",) * (2 * (groups - 1) + 2 * groups + 2)
    units = len(axes)
    dma = pltpu.SemaphoreType.DMA
    bf16, f32 = jnp.bfloat16, jnp.float32
    shapes = [(width, hk)] * 4 + [(width, half)] * (4 * groups - 2) + [(cols, width // 2)] * 2
    out = pl.pallas_call(
        functools.partial(layer_kernel, n, ways, heads, axes),
        out_shape=pltpu.VMEM((rows, width), bf16),
        in_specs=[pl.BlockSpec(memory_space=pltpu.HBM)] * 12,
        out_specs=pl.BlockSpec(memory_space=pltpu.VMEM),
        scratch_shapes=[pltpu.VMEM(shape, bf16) for shape in shapes]
        + [
            pltpu.VMEM(tokens.shape, bf16),
            pltpu.VMEM((1, width), f32),
            pltpu.VMEM(extra_decay.shape, f32),
            pltpu.VMEM((1, cols), f32),
            pltpu.VMEM(initial_state.shape, f32),
            pltpu.VMEM((1, hv), f32),
            pltpu.VMEM((1, width), f32),
            pltpu.VMEM((2 * length, width), f32),
            pltpu.VMEM((rows, width), bf16),
            pltpu.VMEM((rows, cols), bf16),
            pltpu.VMEM((rows, cols), bf16),
            pltpu.VMEM((rows, cols), bf16),
            pltpu.VMEM((rows, cols), bf16),
            pltpu.VMEM((rows, cols), bf16),
            pltpu.VMEM((rows, cols), f32),
            pltpu.VMEM((heads, 1, hk), f32),
            pltpu.VMEM((heads, seqs, hk), f32),
            pltpu.VMEM((heads, seqs, hk), f32),
            pltpu.VMEM((rows, cols), f32),
            pltpu.VMEM((2 * length, cols), bf16),
            pltpu.VMEM((n, own, 128), f32),
            pltpu.VMEM((n, own, 128), f32),
            pltpu.VMEM((n, 128, own), f32),
            pltpu.VMEM((own, hv, hk), bf16),
            pltpu.VMEM((total, 2, hv, hk), bf16),
            pltpu.VMEM((total, hv, hk), bf16),
            pltpu.VMEM((total, 2, hv, hk), bf16),
            pltpu.VMEM((total, hv, hk), bf16),
            pltpu.VMEM((total, hv, hk), bf16),
            pltpu.VMEM((2, groups, seqs, hk), f32),
            pltpu.VMEM((groups, seqs, hk), f32),
            dma((11,)),
            dma((peers,)),
            dma((units, peers)),
            dma((3, peers)),
            dma((units, peers)),
            dma((2, 1 + peers)),
            dma((units,)),
            dma(()),
            dma((n - 1,)),
            dma((own,)),
            dma(()),
            dma((total,)),
            dma(()),
            dma((groups,)),
            dma(()),
            dma((total,)),
            dma(()),
            dma((total,)),
            pltpu.SemaphoreType.REGULAR,
            pltpu.SemaphoreType.REGULAR,
        ],
        compiler_params=pltpu.CompilerParams(
            collective_id=0,
            has_side_effects=True,
            vmem_limit_bytes=67043328 - rows * width * 4 - 2**18,
        ),
        cost_estimate=pl.CostEstimate(
            flops=6 * 10**9, bytes_accessed=2 * 10**7, transcendentals=10**6
        ),
    )(
        tokens,
        pre_gain[None, :],
        w_forget,
        w_value,
        w_query,
        w_gate,
        w_out,
        extra_decay,
        lower_bound[None, :],
        initial_state,
        norm_gain[None, :],
        post_gain[None, :],
    )
    return out.reshape(seqs, length, width)


def solution(mesh):
    in_specs = (
        P("dp", "sp", None),
        P(),
        P("dp", None),
        P("dp", None),
        P("dp", None),
        P("dp", None),
        P(),
        P(("dp", "sp"), None),
        P(("dp", "sp"), None, None),
        P(),
        P("dp", None),
        P(),
    )
    out_specs = P("dp", "sp", None)
    return jax.shard_map(
        functools.partial(body, mesh.shape["sp"], mesh.shape["dp"]),
        mesh=mesh,
        in_specs=in_specs,
        out_specs=out_specs,
        check_vma=False,
    )
```
